32 devices in a mesh: rep: 2 (over x), fs: 8 (over z, y), tp: 2 (over core).
Axes of the slice: x: 2, y: 2, z: 4, core: 2. Of those that a mesh axis runs over, the one named last changes fastest.
Arguments:
- stream_in: bfloat16 [16, 768, 2048], P(('rep', 'fs'), None, 'tp'), may hold values from -6 to 6
- mix_gain: float32 [2048], replicated, may hold values from 0.1 to 1.9
- lin_weight: bfloat16 [2048, 2048], P('fs', 'tp'), may hold values from -0.125 to 0.125
- branch_weight: bfloat16 [2048, 2048], P('fs', 'tp'), may hold values from -0.125 to 0.125
- lin_taps: float32 [4, 2048], P(None, 'tp'), may hold values from -3 to 3
- rate_blocks: bfloat16 [16, 128, 128], P('tp'), may hold values from -0.5 to 0.5
- admit_blocks: bfloat16 [16, 128, 128], P('tp'), may hold values from -0.5 to 0.5
- decay_logit: float32 [2048], P('tp'), may hold values from 3.5 to 9
- mix_out_gain: float32 [2048], P('tp'), may hold values from 0.1 to 1.9
- out_weight: bfloat16 [2048, 2048], P('tp', 'fs'), may hold values from -0.125 to 0.125
- ffn_gain: float32 [2048], replicated, may hold values from 0.1 to 1.9
- gate_weight: bfloat16 [2048, 2816], P('fs', 'tp'), may hold values from -0.125 to 0.125
- up_weight: bfloat16 [2048, 2816], P('fs', 'tp'), may hold values from -0.125 to 0.125
- gate_taps: float32 [3, 2816], P(None, 'tp'), may hold values from -3 to 3
- up_taps: float32 [3, 2816], P(None, 'tp'), may hold values from -3 to 3
- down_weight: bfloat16 [2816, 2048], P('tp', 'fs'), may hold values from -0.109375 to 0.109375
Outputs:
- stream_out: bfloat16 [16, 768, 2048], P(('rep', 'fs'), None, 'tp')
The draws below stay inside these ranges and needn't reach their ends.
All inputs are finite; a program needn't handle non-finite values.
Results may differ from the reference program's by a relative error of at most 0.018.
Values may be sent and summed in bfloat16 or wider, within the bound.
A program may use at most 128 MiB of HBM per device.

```python
import jax
import jax.numpy as jnp
from jax import lax

D = 2048
HD = 128
BLOCKS = 16
FF = 2816
LEN = 768
LRU = 2048
SEQS = 16
N_TP = 2


def steps_of(rng, dims, split, smallest, top_value):
    level = 1.0
    for axis_at, parts in split:
        heights = jax.random.uniform(jax.random.fold_in(jax.random.fold_in(rng, 6), axis_at), (parts,), jnp.float32, smallest / len(split), top_value / len(split))
        level = level * jnp.repeat(jnp.exp(heights), dims[axis_at] // parts).reshape((-1,) + (1,) * (len(dims) - 1 - axis_at))
    return level


def scatter_about(rng, dims, deviation, limit, cuts=(), held_as=jnp.bfloat16):
    level = steps_of(rng, dims, cuts, -0.22, 0.18) if cuts else 1.0
    array = jax.random.normal(rng, dims, jnp.float32) * deviation * level
    return jnp.minimum(jnp.maximum(array, -limit), limit).astype(held_as)


def setup_inputs(seed: int = 0) -> dict:
    streams_of = jax.random.split(jax.random.key(seed), 17)
    return {
        "stream_in": scatter_about(streams_of[0], (SEQS, LEN, D), 1.0, 6.0, ((0, 16), (2, 2))),
        "mix_gain": jnp.clip(1.0 + 0.18 * jax.random.normal(streams_of[1], (D,), jnp.float32), 0.1, 1.9),
        "lin_weight": scatter_about(streams_of[2], (D, LRU), D ** -0.5, 0.125, ((0, 8), (1, 2))),
        "branch_weight": scatter_about(streams_of[3], (D, LRU), D ** -0.5, 0.125, ((0, 8), (1, 2))),
        "lin_taps": scatter_about(streams_of[4], (4, LRU), 0.5, 3.0, ((1, 2),), jnp.float32),
        "rate_blocks": scatter_about(streams_of[5], (BLOCKS, HD, HD), HD ** -0.5, 0.5, ((0, 2),)),
        "admit_blocks": scatter_about(streams_of[6], (BLOCKS, HD, HD), HD ** -0.5, 0.5, ((0, 2),)),
        "decay_logit": jnp.clip(3.5 + 5.5 * jax.random.uniform(streams_of[7], (LRU,), jnp.float32) ** steps_of(streams_of[7], (LRU,), ((0, 2),), -0.2, 0.2), 3.5, 9.0),
        "mix_out_gain": jnp.clip(1.0 + 0.18 * jax.random.normal(streams_of[8], (LRU,), jnp.float32), 0.1, 1.9),
        "out_weight": scatter_about(streams_of[9], (LRU, D), LRU ** -0.5, 0.125, ((0, 2), (1, 8))),
        "ffn_gain": jnp.clip(1.0 + 0.18 * jax.random.normal(streams_of[10], (D,), jnp.float32), 0.1, 1.9),
        "gate_weight": scatter_about(streams_of[11], (D, FF), D ** -0.5, 0.125, ((0, 8), (1, 2))),
        "up_weight": scatter_about(streams_of[12], (D, FF), D ** -0.5, 0.125, ((0, 8), (1, 2))),
        "gate_taps": scatter_about(streams_of[13], (3, FF), 0.6, 3.0, ((1, 2),), jnp.float32),
        "up_taps": scatter_about(streams_of[14], (3, FF), 0.6, 3.0, ((1, 2),), jnp.float32),
        "down_weight": scatter_about(streams_of[15], (FF, D), FF ** -0.5, 0.109375, ((0, 2), (1, 8))),
    }


EPS = 1e-06
GATE_SCALE = 8.0

def norm_rows(values, scales):
    mean_sq = lax.optimization_barrier(jnp.mean(values * values, axis=-1, keepdims=True))
    return values * lax.rsqrt(mean_sq + EPS) * scales

def causal_filter(values, kernel):
    kernel_len = kernel.shape[0]
    seq_len = values.shape[0]
    padded = jnp.pad(values, ((kernel_len - 1, 0), (0, 0)))
    summed = padded[0:seq_len] * kernel[0]
    for offset in range(1, kernel_len):
        summed = summed + padded[offset:offset + seq_len] * kernel[offset]
    return summed

def chain_combine(earlier, later):
    return (earlier[0] * later[0], later[0] * earlier[1] + later[1])

def split_product(left, right):
    group = left.shape[1] // N_TP
    summed = jnp.zeros((left.shape[0], right.shape[1]), jnp.float32)
    for column_part in range(N_TP):
        partial_value = jnp.dot(left[:, column_part * group:(column_part + 1) * group], right[column_part * group:(column_part + 1) * group], preferred_element_type=jnp.float32)
        partial_value = lax.optimization_barrier(partial_value.astype(jnp.bfloat16))
        summed = summed + partial_value.astype(jnp.float32)
    return summed

def reference(stream_in, mix_gain, lin_weight, branch_weight, lin_taps, rate_blocks, admit_blocks, decay_logit, mix_out_gain, out_weight, ffn_gain, gate_weight, up_weight, gate_taps, up_taps, down_weight):

    def one_sequence(sequence):
        stream = sequence.astype(jnp.float32)
        normed = norm_rows(stream, mix_gain).astype(jnp.bfloat16)
        linear = jnp.dot(normed, lin_weight, preferred_element_type=jnp.float32).astype(jnp.bfloat16)
        branch = jnp.dot(normed, branch_weight, preferred_element_type=jnp.float32).astype(jnp.bfloat16)
        filtered = causal_filter(linear.astype(jnp.float32), lin_taps)
        blocks = filtered.astype(jnp.bfloat16).astype(jnp.float32).reshape(LEN, BLOCKS, HD)
        rate_gate = jax.nn.sigmoid(jnp.einsum('lbi,bij->lbj', blocks, rate_blocks.astype(jnp.float32)).reshape(LEN, BLOCKS * HD))
        admitted = jax.nn.sigmoid(jnp.einsum('lbi,bij->lbj', blocks, admit_blocks.astype(jnp.float32)).reshape(LEN, BLOCKS * HD))
        log_decay = -GATE_SCALE * rate_gate * jax.nn.softplus(-decay_logit)
        decay = jnp.exp(log_decay)
        driven = jnp.sqrt(-jnp.expm1(2.0 * log_decay)) * admitted * filtered
        _, states = lax.associative_scan(chain_combine, (decay, driven), axis=0)
        gated = (states * jax.nn.gelu(branch.astype(jnp.float32))).reshape(LEN, BLOCKS, HD)
        gated = gated * lax.rsqrt(lax.optimization_barrier(jnp.mean(gated * gated, axis=-1, keepdims=True)) + EPS)
        mixed = (gated.reshape(LEN, BLOCKS * HD) * mix_out_gain).astype(jnp.bfloat16)
        middle = (stream + split_product(mixed, out_weight)).astype(jnp.bfloat16)
        normed2 = norm_rows(middle.astype(jnp.float32), ffn_gain).astype(jnp.bfloat16)
        gate_pre = jnp.dot(normed2, gate_weight, preferred_element_type=jnp.float32).astype(jnp.bfloat16)
        up_pre = jnp.dot(normed2, up_weight, preferred_element_type=jnp.float32).astype(jnp.bfloat16)
        gate_conv = causal_filter(gate_pre.astype(jnp.float32), gate_taps)
        up_conv = causal_filter(up_pre.astype(jnp.float32), up_taps)
        hidden = (jax.nn.silu(gate_conv) * up_conv).astype(jnp.bfloat16)
        return (middle.astype(jnp.float32) + split_product(hidden, down_weight)).astype(jnp.bfloat16)
    return lax.map(one_sequence, stream_in)
```

```python
import functools

import jax
import jax.numpy as jnp
from jax import lax
from jax.experimental import pallas as pl
from jax.experimental.pallas import tpu as pltpu
from jax.sharding import PartitionSpec as P

EPS = 1e-06
GATE_SCALE = 8.0
MESH = pl.DeviceIdType.MESH
LANES = 256
LINE = 2


def shift_rows(x, d, fill):
    rows = lax.broadcasted_iota(jnp.int32, x.shape, 0)
    return jnp.where(rows < d, fill, pltpu.roll(x, d, 0))


def mixer_body(lin_ref, br_ref, taps_ref, rate_ref, admit_ref, slope_ref, gain_ref, o_ref, a_ref, b_ref):
    length, width = lin_ref.shape
    hd = rate_ref.shape[1]
    linear = lin_ref[...].astype(jnp.float32)
    kernel_len = taps_ref.shape[0]
    filtered = linear * taps_ref[kernel_len - 1 : kernel_len]
    for d in range(1, kernel_len):
        filtered = filtered + shift_rows(linear, d, 0.0) * taps_ref[kernel_len - 1 - d : kernel_len - d]
    narrow = filtered.astype(jnp.bfloat16)
    for j in range(width // hd):
        cols = slice(j * hd, (j + 1) * hd)
        piece = narrow[:, cols]
        rate = jax.nn.sigmoid(jnp.dot(piece, rate_ref[j], preferred_element_type=jnp.float32))
        admit = jax.nn.sigmoid(jnp.dot(piece, admit_ref[j], preferred_element_type=jnp.float32))
        log_decay = rate * slope_ref[:, cols]
        u = 2.0 * log_decay
        decay = jnp.exp(log_decay)
        poly = 1.0 + u * (1.0 / 7.0)
        for c in (6.0, 5.0, 4.0, 3.0, 2.0):
            poly = 1.0 + u * (1.0 / c) * poly
        loss = jnp.where(u > -0.35, -u * poly, 1.0 - decay * decay)
        a = decay
        b = jnp.sqrt(loss) * admit * filtered[:, cols]
        sub = lax.broadcasted_iota(jnp.int32, a.shape, 0) % 8
        for d in (1, 2, 4):
            keep = sub >= d
            pa = jnp.where(keep, pltpu.roll(a, d, 0), 1.0)
            pb = jnp.where(keep, pltpu.roll(b, d, 0), 0.0)
            b = a * pb + b
            a = a * pa
        a_ref[:, cols] = a
        b_ref[:, cols] = b

    def advance(t, carry):
        rows = pl.ds(pl.multiple_of(t * 8, 8), 8)
        s = a_ref[rows, :] * carry + b_ref[rows, :]
        b_ref[rows, :] = s
        return s[7:8, :]

    lax.fori_loop(0, length // 8, advance, jnp.zeros((1, width), jnp.float32), unroll=8)
    for j in range(width // hd):
        cols = slice(j * hd, (j + 1) * hd)
        gated = b_ref[:, cols] * jax.nn.gelu(br_ref[:, cols].astype(jnp.float32))
        scale = lax.rsqrt(jnp.mean(gated * gated, axis=-1, keepdims=True) + EPS)
        o_ref[:, cols] = (gated * scale * gain_ref[:, cols]).astype(o_ref.dtype)


def mixer(linear, branch, taps, rate_blocks, admit_blocks, slope, gain):
    length, channels = linear.shape
    hd = rate_blocks.shape[1]
    per = 2 if rate_blocks.shape[0] % 2 == 0 else 1
    width = per * hd
    wide = pl.BlockSpec((length, width), lambda i: (0, i))
    row = pl.BlockSpec((1, width), lambda i: (0, i))
    blk = pl.BlockSpec((per, hd, hd), lambda i: (i, 0, 0))
    return pl.pallas_call(
        mixer_body,
        grid=(channels // width,),
        in_specs=[wide, wide, pl.BlockSpec((taps.shape[0], width), lambda i: (0, i)), blk, blk, row, row],
        out_specs=wide,
        out_shape=jax.ShapeDtypeStruct((length, channels), jnp.bfloat16),
        scratch_shapes=[pltpu.VMEM((length, width), jnp.float32), pltpu.VMEM((length, width), jnp.float32)],
        cost_estimate=pl.CostEstimate(flops=length * channels * 20000, bytes_accessed=length * channels * 6, transcendentals=0),
        name="mixer",
    )(linear, branch, taps, rate_blocks, admit_blocks, slope, gain)


def ffn_body(g_ref, u_ref, gt_ref, ut_ref, o_ref):
    def conv(ref, taps):
        x = ref[...].astype(jnp.float32)
        n = taps.shape[0]
        y = x * taps[n - 1 : n]
        for d in range(1, n):
            y = y + shift_rows(x, d, 0.0) * taps[n - 1 - d : n - d]
        return y

    o_ref[...] = (jax.nn.silu(conv(g_ref, gt_ref)) * conv(u_ref, ut_ref)).astype(o_ref.dtype)


def ffn_gate(gate_pre, up_pre, gate_taps, up_taps):
    length, units = gate_pre.shape
    width = 128
    wide = pl.BlockSpec((length, width), lambda i: (0, i))
    tap = pl.BlockSpec((gate_taps.shape[0], width), lambda i: (0, i))
    return pl.pallas_call(
        ffn_body,
        grid=(units // width,),
        in_specs=[wide, wide, tap, tap],
        out_specs=wide,
        out_shape=jax.ShapeDtypeStruct((length, units), jnp.bfloat16),
        cost_estimate=pl.CostEstimate(flops=length * units * 8000, bytes_accessed=length * units * 6, transcendentals=0),
        name="ffn_gate",
    )(gate_pre, up_pre, gate_taps, up_taps)


def halves(rows):
    first = -(-rows // 256) * 128
    return ((0, first), (first, rows - first))


def plan(shards):
    pieces = []
    for group in ((0, 1), (2,), (3, 4), (5,)):
        for h in range(2):
            for m in group:
                rows = shards[m].shape[0] if m not in (2, 5) else shards[m].shape[0]
                pieces.append((m,) + halves(rows)[h])
    return pieces


def nearest(depth):
    return [sorted(range(depth), key=lambda s: (abs(s - z), -s)) for z in range(depth)]


def choose(values, at):
    out = jnp.int32(values[0])
    for i, v in enumerate(values[1:], 1):
        out = jnp.where(at == i, jnp.int32(v), out)
    return out


def layer_body(depth, pieces, across, x_ref, mix_gain, lin_hbm, br_hbm, taps_ref, rate_ref, admit_ref, slope_ref,
               mix_out_gain, out_hbm, ffn_gain, gate_hbm, up_hbm, gtap_ref, utap_ref, down_hbm, o_ref,
               w_lin, w_br, w_out, w_gate, w_up, w_down, peer, normed, mixed, kept, sent, got, middle, hidden,
               a_ref, b_ref, local_sem, z_send, z_extra, z_recv, y_send, y_recv, p_send, p_recv, q_send, q_recv,
               pair_send, pair_recv, sum_send, sum_recv, end_send, end_recv):
    x = lax.axis_index("rep")
    f_own = lax.axis_index("fs")
    tp = lax.axis_index("tp")
    z, y = f_own // LINE, f_own % LINE
    length, share = x_ref.shape
    order = nearest(depth)
    hbm = (lin_hbm, br_hbm, out_hbm, gate_hbm, up_hbm, down_hbm)
    full = (w_lin, w_br, w_out, w_gate, w_up, w_down)
    flat = tuple(len(w.shape) == 2 for w in full)

    def line(s, row):
        return s * LINE + row

    def near(k):
        return choose([order[i][k] for i in range(depth)], z)

    def view(p, f, start, size):
        m, row0, _ = pieces[p]
        start = pl.multiple_of(row0 + start, 16)
        if flat[m]:
            return full[m].at[pl.ds(pl.multiple_of(f * hbm[m].shape[0] + start, 16), size), :]
        return full[m].at[f, pl.ds(start, size), :]

    def parts(p):
        q, v = pieces[p][2] // 8, across[p]
        return {
            "z": (2 * q * x, 6 * q),
            "y": ((8 - v) * q * x, v * q),
            "p_out": (6 * q * x, 2 * q),
            "p_in": (6 * q * (1 - x), 2 * q),
            "q_out": (v * q * x, (8 - v) * q),
            "q_in": (v * q * (1 - x), (8 - v) * q),
        }

    def push(p, f, part, send, recv, device):
        ref = view(p, f, *parts(p)[part])
        return pltpu.make_async_remote_copy(
            src_ref=ref, dst_ref=ref, send_sem=send, recv_sem=recv, device_id=device, device_id_type=MESH
        )

    def own_copy(m):
        dst = full[m].at[pl.ds(pl.multiple_of(f_own * hbm[m].shape[0], 16), hbm[m].shape[0]), :] if flat[m] else full[m].at[f_own]
        return pltpu.make_async_copy(hbm[m], dst, local_sem.at[m])

    def own(p):
        m, row0, _ = pieces[p]
        if row0 == 0:
            own_copy(m).wait()

        @pl.when(z < depth - 1)
        def _():
            push(p, f_own, "z", z_send.at[p, z], z_recv.at[p, z], {"fs": line(z + 1, y)}).start()

        @pl.when(z > 0)
        def _():
            push(p, f_own, "z", z_extra.at[p], z_recv.at[p, z], {"fs": line(z - 1, y)}).start()

        push(p, f_own, "y", y_send.at[p, z], y_recv.at[p, z], {"fs": line(z, 1 - y)}).start()

    def along(p, k):
        s = near(k)
        f = line(s, y)
        push(p, f, "z", z_send.at[p, s], z_recv.at[p, s], {"fs": f_own}).wait_recv()
        onward = jnp.where(s < z, z + 1, z - 1)

        @pl.when(jnp.logical_and(onward >= 0, onward < depth))
        def _():
            push(p, f, "z", z_send.at[p, s], z_recv.at[p, s], {"fs": line(onward, y)}).start()

        push(p, f, "y", y_send.at[p, s], y_recv.at[p, s], {"fs": line(z, 1 - y)}).start()
        push(p, f, "p_out", p_send.at[p, s], p_recv.at[p, s], {"rep": 1 - x}).start()

    def over(p, k):
        s = near(k)
        f = line(s, 1 - y)
        push(p, f, "y", y_send.at[p, s], y_recv.at[p, s], {"fs": f_own}).wait_recv()
        push(p, f, "q_out", q_send.at[p, s], q_recv.at[p, s], {"rep": 1 - x}).start()

    def landed(p, k):
        s = near(k)
        if k:
            push(p, line(s, y), "p_in", p_send.at[p, s], p_recv.at[p, s], {"rep": 1 - x}).wait_recv()

    def landed_across(p, k):
        s = near(k)
        push(p, line(s, 1 - y), "q_in", q_send.at[p, s], q_recv.at[p, s], {"rep": 1 - x}).wait_recv()

    def complete(m):
        for p, piece in enumerate(pieces):
            if piece[0] == m:
                for k in range(depth):
                    landed(p, k)
                    landed_across(p, k)

    def drain(p):
        @pl.when(z < depth - 1)
        def _():
            push(p, f_own, "z", z_send.at[p, z], z_recv.at[p, z], {"fs": f_own}).wait_send()

        @pl.when(z > 0)
        def _():
            push(p, f_own, "z", z_extra.at[p], z_recv.at[p, z], {"fs": f_own}).wait_send()

        for k in range(depth):
            s = near(k)
            f = line(s, y)
            push(p, f, "y", y_send.at[p, s], y_recv.at[p, s], {"fs": f_own}).wait_send()
            push(p, line(s, 1 - y), "q_out", q_send.at[p, s], q_recv.at[p, s], {"fs": f_own}).wait_send()
            if k:
                push(p, f, "p_out", p_send.at[p, s], p_recv.at[p, s], {"fs": f_own}).wait_send()
                onward = jnp.where(s < z, z + 1, z - 1)

                @pl.when(jnp.logical_and(onward >= 0, onward < depth))
                def _():
                    push(p, f, "z", z_send.at[p, s], z_recv.at[p, s], {"fs": f_own}).wait_send()

    count = len(pieces)

    def stage(p):
        events = [functools.partial(own, p + 2)] if p + 2 < count else []
        for k in range(depth):
            events.append(functools.partial(over, p, k))
            if p + 1 < count and k + 1 < depth:
                events.append(functools.partial(along, p + 1, k + 1))
        return events

    def last_of(m):
        return max(p for p, piece in enumerate(pieces) if piece[0] == m)

    def run(events):
        for event in events:
            event()

    def slots(step, steps, slot, per, events):
        for i in range(steps):
            chosen = events[(i * per + slot) * len(events) // (steps * per) : (i * per + slot + 1) * len(events) // (steps * per)]
            if chosen:
                pl.when(step == i)(functools.partial(run, chosen))

    def pair_copy(i, src, dst):
        return pltpu.make_async_remote_copy(
            src_ref=src, dst_ref=dst, send_sem=pair_send.at[i], recv_sem=pair_recv.at[i],
            device_id={"tp": 1 - tp}, device_id_type=MESH,
        )

    def normalize(mine, gain):
        def chunk(i, carry):
            rows = pl.ds(pl.multiple_of(i * 128, 128), 128)
            a = mine[rows, :].astype(jnp.float32)
            b = peer[rows, :].astype(jnp.float32)
            total = jnp.sum(a * a, axis=-1, keepdims=True) + jnp.sum(b * b, axis=-1, keepdims=True)
            scale = lax.rsqrt(total / (2 * share) + EPS)
            here = pl.ds(pl.multiple_of(tp * share, LANES), share)
            there = pl.ds(pl.multiple_of((1 - tp) * share, LANES), share)
            normed[rows, here] = (a * scale * gain[pl.ds(tp, 1), :]).astype(jnp.bfloat16)
            normed[rows, there] = (b * scale * gain[pl.ds(1 - tp, 1), :]).astype(jnp.bfloat16)
            return carry

        lax.fori_loop(0, length // 128, chunk, 0)

    def project(left, right):
        return jnp.dot(left, right, preferred_element_type=jnp.float32).astype(jnp.bfloat16)

    def mix(j, events, steps):
        cols = pl.ds(pl.multiple_of(j * LANES, LANES), LANES)
        hd = rate_ref.shape[1]
        slots(j, steps, 0, 3, events)
        linear = project(normed[...], w_lin[:, cols]).astype(jnp.float32)
        kernel_len = taps_ref.shape[0]
        filtered = linear * taps_ref[kernel_len - 1 : kernel_len, cols]
        for d in range(1, kernel_len):
            filtered = filtered + shift_rows(linear, d, 0.0) * taps_ref[kernel_len - 1 - d : kernel_len - d, cols]
        narrow = filtered.astype(jnp.bfloat16)
        for i in range(LANES // hd):
            part = slice(i * hd, (i + 1) * hd)
            lanes = pl.ds(pl.multiple_of(j * LANES + i * hd, hd), hd)
            block = j * (LANES // hd) + i
            piece = narrow[:, part]
            rate = jax.nn.sigmoid(jnp.dot(piece, rate_ref[block], preferred_element_type=jnp.float32))
            admit = jax.nn.sigmoid(jnp.dot(piece, admit_ref[block], preferred_element_type=jnp.float32))
            log_decay = rate * slope_ref[:, lanes]
            u = 2.0 * log_decay
            a = jnp.exp(log_decay)
            poly = 1.0 + u * (1.0 / 7.0)
            for c in (6.0, 5.0, 4.0, 3.0, 2.0):
                poly = 1.0 + u * (1.0 / c) * poly
            loss = jnp.where(u > -0.35, -u * poly, 1.0 - a * a)
            b = jnp.sqrt(loss) * admit * filtered[:, part]
            sub = lax.broadcasted_iota(jnp.int32, a.shape, 0) % 8
            for d in (1, 2, 4):
                keep = sub >= d
                pa = jnp.where(keep, pltpu.roll(a, d, 0), 1.0)
                pb = jnp.where(keep, pltpu.roll(b, d, 0), 0.0)
                b = a * pb + b
                a = a * pa
            a_ref[:, part] = a
            b_ref[:, part] = b
        slots(j, steps, 1, 3, events)

        def advance(t, carry):
            rows = pl.ds(pl.multiple_of(t * 8, 8), 8)
            s = a_ref[rows, :] * carry + b_ref[rows, :]
            b_ref[rows, :] = s
            return s[7:8, :]

        lax.fori_loop(0, length // 8, advance, jnp.zeros((1, LANES), jnp.float32), unroll=8)
        slots(j, steps, 2, 3, events)
        branch = project(normed[...], w_br[:, cols])
        for i in range(LANES // hd):
            part = slice(i * hd, (i + 1) * hd)
            lanes = pl.ds(pl.multiple_of(j * LANES + i * hd, hd), hd)
            gated = b_ref[:, part] * jax.nn.gelu(branch[:, part].astype(jnp.float32))
            scale = lax.rsqrt(jnp.mean(gated * gated, axis=-1, keepdims=True) + EPS)
            mixed[:, lanes] = (gated * scale * mix_out_gain[:, lanes]).astype(mixed.dtype)

    def feed(col, width):
        cols = pl.ds(col, width)

        def conv(weight, taps):
            v = project(normed[...], weight[:, cols]).astype(jnp.float32)
            n = taps.shape[0]
            out = v * taps[n - 1 : n, cols]
            for d in range(1, n):
                out = out + shift_rows(v, d, 0.0) * taps[n - 1 - d : n - d, cols]
            return out

        hidden[:, cols] = (jax.nn.silu(conv(w_gate, gtap_ref)) * conv(w_up, utap_ref)).astype(hidden.dtype)

    per = kept.shape[0]

    def share_out(f, left, weight, send, recv):
        result = project(left[...], weight[f])
        slot = f % per

        @pl.when(f // per == tp)
        def _():
            kept[slot] = result

        @pl.when(f // per != tp)
        def _():
            sent[slot] = result
            part_copy(slot, send, recv).start()

    def part_copy(slot, send, recv):
        return pltpu.make_async_remote_copy(
            src_ref=sent.at[slot], dst_ref=got.at[slot], send_sem=send.at[slot], recv_sem=recv.at[slot],
            device_id={"tp": 1 - tp}, device_id_type=MESH,
        )

    def add_up(base, target, send, recv):
        for i in range(per):
            cols = slice(i * LANES, (i + 1) * LANES)
            part_copy(i, send, recv).wait_recv()
            total = kept[i].astype(jnp.float32) + got[i].astype(jnp.float32)
            target[:, cols] = (base[:, cols].astype(jnp.float32) + total).astype(target.dtype)
        for i in range(per):
            part_copy(i, send, recv).wait_send()

    for m in range(6):
        own_copy(m).start()
    barrier = pltpu.get_barrier_semaphore()
    for device in ({"rep": 1 - x}, {"fs": line(z, 1 - y)}, {"tp": 1 - tp}):
        pl.semaphore_signal(barrier, inc=1, device_id=device, device_id_type=MESH)

    @pl.when(z > 0)
    def _():
        pl.semaphore_signal(barrier, inc=1, device_id={"fs": line(z - 1, y)}, device_id_type=MESH)

    @pl.when(z < depth - 1)
    def _():
        pl.semaphore_signal(barrier, inc=1, device_id={"fs": line(z + 1, y)}, device_id_type=MESH)

    pl.semaphore_wait(barrier, 3 + jnp.where(z > 0, 1, 0) + jnp.where(z < depth - 1, 1, 0))

    own(0)
    own(1)
    pair_copy(0, x_ref, peer).start()
    along(0, 1)
    pair_copy(0, x_ref, peer).wait()
    normalize(x_ref, mix_gain)
    for k in range(2, depth):
        along(0, k)
    at = 0
    while at <= last_of(1):
        run(stage(at))
        at += 1
    complete(0)
    complete(1)
    later = []
    while at <= last_of(2):
        later += stage(at)
        at += 1
    steps = share // LANES
    pl.loop(0, steps)(lambda j: mix(j, later, steps))
    complete(2)
    later = stage(at)
    at += 1

    @pl.loop(0, 2 * per)
    def _(f):
        slots(f, 2 * per, 0, 1, later)
        share_out(f, mixed, w_out, sum_send, sum_recv)

    add_up(x_ref, middle, sum_send, sum_recv)
    pair_copy(1, middle, peer).start()
    later = stage(at)
    at += 1
    run(later[: len(later) // 2])
    pair_copy(1, middle, peer).wait()
    normalize(middle, ffn_gain)
    run(later[len(later) // 2 :])
    while at <= last_of(4):
        run(stage(at))
        at += 1
    complete(3)
    complete(4)
    later = []
    while at < count:
        later += stage(at)
        at += 1
    units = hidden.shape[1]
    wide = units // LANES
    first = len(later) * wide // (wide + 1) if units % LANES else len(later)

    @pl.loop(0, wide)
    def _(j):
        slots(j, wide, 0, 1, later[:first])
        feed(pl.multiple_of(j * LANES, LANES), LANES)

    if units % LANES:
        feed(wide * LANES, units % LANES)
    run(later[first:])

    @pl.loop(0, 2 * depth)
    def _(t):
        for k in range(depth):
            for side, waits in enumerate((landed, landed_across)):
                @pl.when(t == 2 * k + side)
                def _():
                    for p, piece in enumerate(pieces):
                        if piece[0] == 5:
                            waits(p, k)
        s = choose([order[i][0] for i in range(depth)], z)
        for k in range(1, depth):
            s = jnp.where(t // 2 == k, near(k), s)
        f = jnp.where(t % 2 == 0, line(s, y), line(s, 1 - y))
        share_out(f, hidden, w_down, end_send, end_recv)

    add_up(middle, o_ref, end_send, end_recv)
    for p in range(count):
        drain(p)


def fused(depth, stream_in, mix_gain, lin_weight, branch_weight, lin_taps, rate_blocks, admit_blocks, decay_logit,
          mix_out_gain, out_weight, ffn_gain, gate_weight, up_weight, gate_taps, up_taps, down_weight):
    own = stream_in[0]
    length, share = own.shape
    n = LINE * depth
    shards = (lin_weight, branch_weight, out_weight, gate_weight, up_weight, down_weight)
    pieces = plan(shards)
    across = [4 if m == 5 else 5 for m, _, _ in pieces]
    slope = (-GATE_SCALE * jax.nn.softplus(-decay_logit)).reshape(1, -1)
    bf = jnp.bfloat16
    whole = [
        pltpu.VMEM((n,) + w.shape, bf) if m in (2, 5) else pltpu.VMEM((n * w.shape[0], w.shape[1]), bf)
        for m, w in enumerate(shards)
    ]
    units = gate_weight.shape[1]
    channels = lin_weight.shape[1]
    width = out_weight.shape[1]
    count = len(pieces)
    dma = pltpu.SemaphoreType.DMA
    scratch = whole + [
        pltpu.VMEM((length, share), bf),
        pltpu.VMEM((length, 2 * share), bf),
        pltpu.VMEM((length, channels), bf),
        pltpu.VMEM((n // 2, length, width), bf),
        pltpu.VMEM((n // 2, length, width), bf),
        pltpu.VMEM((n // 2, length, width), bf),
        pltpu.VMEM((length, share), bf),
        pltpu.VMEM((length, units), bf),
        pltpu.VMEM((length, LANES), jnp.float32),
        pltpu.VMEM((length, LANES), jnp.float32),
        dma((6,)),
        dma((count, depth)),
        dma((count,)),
        dma((count, depth)),
        dma((count, depth)),
        dma((count, depth)),
        dma((count, depth)),
        dma((count, depth)),
        dma((count, depth)),
        dma((count, depth)),
        dma((2,)),
        dma((2,)),
        dma((n // 2,)),
        dma((n // 2,)),
        dma((n // 2,)),
        dma((n // 2,)),
    ]
    near = pl.BlockSpec(memory_space=pltpu.VMEM)
    far = pl.BlockSpec(memory_space=pl.ANY)
    macs = length * share * 2 * (3 * share + 3 * units)
    result = pl.pallas_call(
        functools.partial(layer_body, depth, pieces, across),
        in_specs=[near, near, far, far, near, near, near, near, near, far, near, far, far, near, near, far],
        out_specs=near,
        out_shape=jax.ShapeDtypeStruct((length, share), bf),
        scratch_shapes=scratch,
        compiler_params=pltpu.CompilerParams(collective_id=0, has_side_effects=True, vmem_limit_bytes=67043328),
        cost_estimate=pl.CostEstimate(flops=2 * macs, bytes_accessed=2 * macs // length, transcendentals=0),
        name="layer",
    )(own, mix_gain.reshape(2, share), lin_weight, branch_weight, lin_taps, rate_blocks, admit_blocks, slope,
      mix_out_gain.reshape(1, -1), out_weight, ffn_gain.reshape(2, share), gate_weight, up_weight, gate_taps,
      up_taps, down_weight)
    return result[None]


def gathered(tps, stream_in, mix_gain, lin_weight, branch_weight, lin_taps, rate_blocks, admit_blocks,
             decay_logit, mix_out_gain, out_weight, ffn_gain, gate_weight, up_weight, gate_taps, up_taps, down_weight):
    own = stream_in[0]
    length, share = own.shape

    def normed_rows(mine, gain):
        pair = lax.all_gather(mine, "tp", axis=0).astype(jnp.float32)
        mean_sq = jnp.sum(pair * pair, axis=(0, 2), keepdims=True) / (tps * share)
        y = (pair * lax.rsqrt(mean_sq + EPS) * gain.reshape(tps, 1, share)).astype(jnp.bfloat16)
        return y.transpose(1, 0, 2).reshape(length, tps * share)

    def product(left, right):
        return jnp.dot(left, right, preferred_element_type=jnp.float32).astype(jnp.bfloat16)

    def scatter(left, right):
        stack = product(left, right).reshape(length, tps, share).transpose(1, 0, 2)
        if tps == 2:
            tp = lax.axis_index("tp")
            mine = lax.dynamic_index_in_dim(stack, tp, 0, keepdims=False)
            other = lax.dynamic_index_in_dim(stack, 1 - tp, 0, keepdims=False)
            other = lax.ppermute(other, "tp", [(0, 1), (1, 0)])
            return mine.astype(jnp.float32) + other.astype(jnp.float32)
        return lax.psum_scatter(stack, "tp", scatter_dimension=0, tiled=False).astype(jnp.float32)

    def gather(w, axis=0):
        return lax.all_gather(w, "fs", axis=axis, tiled=True)

    normed = normed_rows(own, mix_gain)
    linear = product(normed, gather(lin_weight))
    branch = product(normed, gather(branch_weight))
    slope = (-GATE_SCALE * jax.nn.softplus(-decay_logit)).reshape(1, -1)
    mixed = mixer(linear, branch, lin_taps, rate_blocks, admit_blocks, slope, mix_out_gain.reshape(1, -1))
    middle = (own.astype(jnp.float32) + scatter(mixed, gather(out_weight, 1))).astype(jnp.bfloat16)
    normed2 = normed_rows(middle, ffn_gain)
    gate_pre = product(normed2, gather(gate_weight))
    up_pre = product(normed2, gather(up_weight))
    hidden = ffn_gate(gate_pre, up_pre, gate_taps, up_taps)
    result = (middle.astype(jnp.float32) + scatter(hidden, gather(down_weight, 1))).astype(jnp.bfloat16)
    return result[None]


def solution(mesh):
    placed = (
        P(("rep", "fs"), None, "tp"),
        P(),
        P("fs", "tp"),
        P("fs", "tp"),
        P(None, "tp"),
        P("tp", None, None),
        P("tp", None, None),
        P("tp"),
        P("tp"),
        P("tp", "fs"),
        P(),
        P("fs", "tp"),
        P("fs", "tp"),
        P(None, "tp"),
        P(None, "tp"),
        P("tp", "fs"),
    )
    reps, n, tps = mesh.shape["rep"], mesh.shape["fs"], mesh.shape["tp"]
    if reps == 2 and tps == 2 and n == 8:
        body = functools.partial(fused, n // LINE)
    else:
        body = functools.partial(gathered, tps)
    return jax.shard_map(
        body, mesh=mesh, in_specs=placed, out_specs=P(("rep", "fs"), None, "tp"), check_vma=False
    )
```

```python
import functools

import jax
import jax.numpy as jnp
from jax import lax
from jax.experimental import pallas as pl
from jax.experimental.pallas import tpu as pltpu
from jax.sharding import PartitionSpec as P

EPS = 1e-06
GATE_SCALE = 8.0
MESH = pl.DeviceIdType.MESH
LANES = 256
LINE = 2


def shift_rows(x, d, fill):
    rows = lax.broadcasted_iota(jnp.int32, x.shape, 0)
    return jnp.where(rows < d, fill, pltpu.roll(x, d, 0))


def mixer_body(lin_ref, br_ref, taps_ref, rate_ref, admit_ref, slope_ref, gain_ref, o_ref, a_ref, b_ref):
    length, width = lin_ref.shape
    hd = rate_ref.shape[1]
    linear = lin_ref[...].astype(jnp.float32)
    kernel_len = taps_ref.shape[0]
    filtered = linear * taps_ref[kernel_len - 1 : kernel_len]
    for d in range(1, kernel_len):
        filtered = filtered + shift_rows(linear, d, 0.0) * taps_ref[kernel_len - 1 - d : kernel_len - d]
    narrow = filtered.astype(jnp.bfloat16)
    for j in range(width // hd):
        cols = slice(j * hd, (j + 1) * hd)
        piece = narrow[:, cols]
        rate = jax.nn.sigmoid(jnp.dot(piece, rate_ref[j], preferred_element_type=jnp.float32))
        admit = jax.nn.sigmoid(jnp.dot(piece, admit_ref[j], preferred_element_type=jnp.float32))
        log_decay = rate * slope_ref[:, cols]
        u = 2.0 * log_decay
        decay = jnp.exp(log_decay)
        poly = 1.0 + u * (1.0 / 7.0)
        for c in (6.0, 5.0, 4.0, 3.0, 2.0):
            poly = 1.0 + u * (1.0 / c) * poly
        loss = jnp.where(u > -0.35, -u * poly, 1.0 - decay * decay)
        a = decay
        b = jnp.sqrt(loss) * admit * filtered[:, cols]
        sub = lax.broadcasted_iota(jnp.int32, a.shape, 0) % 8
        for d in (1, 2, 4):
            keep = sub >= d
            pa = jnp.where(keep, pltpu.roll(a, d, 0), 1.0)
            pb = jnp.where(keep, pltpu.roll(b, d, 0), 0.0)
            b = a * pb + b
            a = a * pa
        a_ref[:, cols] = a
        b_ref[:, cols] = b

    def advance(t, carry):
        rows = pl.ds(pl.multiple_of(t * 8, 8), 8)
        s = a_ref[rows, :] * carry + b_ref[rows, :]
        b_ref[rows, :] = s
        return s[7:8, :]

    lax.fori_loop(0, length // 8, advance, jnp.zeros((1, width), jnp.float32), unroll=8)
    for j in range(width // hd):
        cols = slice(j * hd, (j + 1) * hd)
        gated = b_ref[:, cols] * jax.nn.gelu(br_ref[:, cols].astype(jnp.float32))
        scale = lax.rsqrt(jnp.mean(gated * gated, axis=-1, keepdims=True) + EPS)
        o_ref[:, cols] = (gated * scale * gain_ref[:, cols]).astype(o_ref.dtype)


def mixer(linear, branch, taps, rate_blocks, admit_blocks, slope, gain):
    length, channels = linear.shape
    hd = rate_blocks.shape[1]
    per = 2 if rate_blocks.shape[0] % 2 == 0 else 1
    width = per * hd
    wide = pl.BlockSpec((length, width), lambda i: (0, i))
    row = pl.BlockSpec((1, width), lambda i: (0, i))
    blk = pl.BlockSpec((per, hd, hd), lambda i: (i, 0, 0))
    return pl.pallas_call(
        mixer_body,
        grid=(channels // width,),
        in_specs=[wide, wide, pl.BlockSpec((taps.shape[0], width), lambda i: (0, i)), blk, blk, row, row],
        out_specs=wide,
        out_shape=jax.ShapeDtypeStruct((length, channels), jnp.bfloat16),
        scratch_shapes=[pltpu.VMEM((length, width), jnp.float32), pltpu.VMEM((length, width), jnp.float32)],
        cost_estimate=pl.CostEstimate(flops=length * channels * 20000, bytes_accessed=length * channels * 6, transcendentals=0),
        name="mixer",
    )(linear, branch, taps, rate_blocks, admit_blocks, slope, gain)


def ffn_body(g_ref, u_ref, gt_ref, ut_ref, o_ref):
    def conv(ref, taps):
        x = ref[...].astype(jnp.float32)
        n = taps.shape[0]
        y = x * taps[n - 1 : n]
        for d in range(1, n):
            y = y + shift_rows(x, d, 0.0) * taps[n - 1 - d : n - d]
        return y

    o_ref[...] = (jax.nn.silu(conv(g_ref, gt_ref)) * conv(u_ref, ut_ref)).astype(o_ref.dtype)


def ffn_gate(gate_pre, up_pre, gate_taps, up_taps):
    length, units = gate_pre.shape
    width = 128
    wide = pl.BlockSpec((length, width), lambda i: (0, i))
    tap = pl.BlockSpec((gate_taps.shape[0], width), lambda i: (0, i))
    return pl.pallas_call(
        ffn_body,
        grid=(units // width,),
        in_specs=[wide, wide, tap, tap],
        out_specs=wide,
        out_shape=jax.ShapeDtypeStruct((length, units), jnp.bfloat16),
        cost_estimate=pl.CostEstimate(flops=length * units * 8000, bytes_accessed=length * units * 6, transcendentals=0),
        name="ffn_gate",
    )(gate_pre, up_pre, gate_taps, up_taps)


SPLIT = (
    ((4, 4), (6, 4)),
    ((6, 6), (4, 4)),
    ((8, 5), (4, 4)),
    ((6, 4), (7, 4)),
    ((6, 6), (7, 6)),
    ((7, 5), (7, 4), (7, 4), (8, 5)),
)
CUTS = (5, 7, 8, 9, 11)


def plan(shards):
    cuts = []
    for m, w in enumerate(shards):
        rows, parts = w.shape[0], len(SPLIT[m])
        step = -(-rows // (128 * parts)) * 128
        cuts.append([(m, at, min(step, rows - at)) + SPLIT[m][i] for i, at in enumerate(range(0, rows, step))])
    pieces = []
    for group in ((0, 1), (2,), (3, 4), (5,)):
        for i in range(max(len(cuts[m]) for m in group)):
            pieces += [cuts[m][i] for m in group if i < len(cuts[m])]
    return pieces


def nearest(depth):
    return [sorted(range(depth), key=lambda s: (abs(s - z), -s)) for z in range(depth)]


def choose(values, at):
    out = jnp.int32(values[0])
    for i, v in enumerate(values[1:], 1):
        out = jnp.where(at == i, jnp.int32(v), out)
    return out


def layer_body(depth, pieces, x_ref, mix_gain, lin_hbm, br_hbm, taps_ref, rate_ref, admit_ref, logit_ref,
               mix_out_gain, out_hbm, ffn_gain, gate_hbm, up_hbm, gtap_ref, utap_ref, down_hbm, o_ref,
               w_lin, w_br, w_out, w_gate, w_up, w_down, peer, normed, mixed, kept, sent, got, middle, hidden,
               a_ref, b_ref, local_sem, z_send, z_extra, z_recv, y_send, y_recv, p_send, p_recv, q_send, q_recv,
               pair_send, pair_recv, sum_send, sum_recv, end_send, end_recv):
    x = lax.axis_index("rep")
    f_own = lax.axis_index("fs")
    tp = lax.axis_index("tp")
    z, y = f_own // LINE, f_own % LINE
    length, share = x_ref.shape
    order = nearest(depth)
    hbm = (lin_hbm, br_hbm, out_hbm, gate_hbm, up_hbm, down_hbm)
    full = (w_lin, w_br, w_out, w_gate, w_up, w_down)
    flat = tuple(len(w.shape) == 2 for w in full)

    def line(s, row):
        return s * LINE + row

    def near(k):
        return choose([order[i][k] for i in range(depth)], z)

    def view(p, f, start, size):
        m, row0 = pieces[p][:2]
        start = pl.multiple_of(row0 + start, 16)
        if flat[m]:
            return full[m].at[pl.ds(pl.multiple_of(f * hbm[m].shape[0] + start, 16), size), :]
        return full[m].at[f, pl.ds(start, size), :]

    def parts(p):
        q, (u, v) = pieces[p][2] // 8, pieces[p][3:]
        return {
            "z": ((8 - u) * q * x, u * q),
            "y": ((8 - v) * q * x, v * q),
            "p_out": (u * q * x, (8 - u) * q),
            "p_in": (u * q * (1 - x), (8 - u) * q),
            "q_out": (v * q * x, (8 - v) * q),
            "q_in": (v * q * (1 - x), (8 - v) * q),
        }

    def spare(p, side):
        return pieces[p][3 + side] < 8

    def push(p, f, part, send, recv, device):
        ref = view(p, f, *parts(p)[part])
        return pltpu.make_async_remote_copy(
            src_ref=ref, dst_ref=ref, send_sem=send, recv_sem=recv, device_id=device, device_id_type=MESH
        )

    def own_copy(m):
        dst = full[m].at[pl.ds(pl.multiple_of(f_own * hbm[m].shape[0], 16), hbm[m].shape[0]), :] if flat[m] else full[m].at[f_own]
        return pltpu.make_async_copy(hbm[m], dst, local_sem.at[m])

    def own(p):
        m, row0 = pieces[p][:2]
        if row0 == 0:
            own_copy(m).wait()

        @pl.when(z < depth - 1)
        def _():
            push(p, f_own, "z", z_send.at[p, z], z_recv.at[p, z], {"fs": line(z + 1, y)}).start()

        @pl.when(z > 0)
        def _():
            push(p, f_own, "z", z_extra.at[p], z_recv.at[p, z], {"fs": line(z - 1, y)}).start()

        push(p, f_own, "y", y_send.at[p, z], y_recv.at[p, z], {"fs": line(z, 1 - y)}).start()

    def along(p, k):
        s = near(k)
        f = line(s, y)
        push(p, f, "z", z_send.at[p, s], z_recv.at[p, s], {"fs": f_own}).wait_recv()
        onward = jnp.where(s < z, z + 1, z - 1)

        @pl.when(jnp.logical_and(onward >= 0, onward < depth))
        def _():
            push(p, f, "z", z_send.at[p, s], z_recv.at[p, s], {"fs": line(onward, y)}).start()

        push(p, f, "y", y_send.at[p, s], y_recv.at[p, s], {"fs": line(z, 1 - y)}).start()
        if spare(p, 0):
            push(p, f, "p_out", p_send.at[p, s], p_recv.at[p, s], {"rep": 1 - x}).start()

    def over(p, k):
        s = near(k)
        f = line(s, 1 - y)
        push(p, f, "y", y_send.at[p, s], y_recv.at[p, s], {"fs": f_own}).wait_recv()
        if spare(p, 1):
            push(p, f, "q_out", q_send.at[p, s], q_recv.at[p, s], {"rep": 1 - x}).start()

    def landed(p, k):
        s = near(k)
        if k and spare(p, 0):
            push(p, line(s, y), "p_in", p_send.at[p, s], p_recv.at[p, s], {"rep": 1 - x}).wait_recv()

    def landed_across(p, k):
        s = near(k)
        if spare(p, 1):
            push(p, line(s, 1 - y), "q_in", q_send.at[p, s], q_recv.at[p, s], {"rep": 1 - x}).wait_recv()

    def complete(m):
        for p, piece in enumerate(pieces):
            if piece[0] == m:
                for k in range(depth):
                    landed(p, k)
                    landed_across(p, k)

    def drain(p):
        @pl.when(z < depth - 1)
        def _():
            push(p, f_own, "z", z_send.at[p, z], z_recv.at[p, z], {"fs": f_own}).wait_send()

        @pl.when(z > 0)
        def _():
            push(p, f_own, "z", z_extra.at[p], z_recv.at[p, z], {"fs": f_own}).wait_send()

        for k in range(depth):
            s = near(k)
            f = line(s, y)
            push(p, f, "y", y_send.at[p, s], y_recv.at[p, s], {"fs": f_own}).wait_send()
            if spare(p, 1):
                push(p, line(s, 1 - y), "q_out", q_send.at[p, s], q_recv.at[p, s], {"fs": f_own}).wait_send()
            if k:
                if spare(p, 0):
                    push(p, f, "p_out", p_send.at[p, s], p_recv.at[p, s], {"fs": f_own}).wait_send()
                onward = jnp.where(s < z, z + 1, z - 1)

                @pl.when(jnp.logical_and(onward >= 0, onward < depth))
                def _():
                    push(p, f, "z", z_send.at[p, s], z_recv.at[p, s], {"fs": f_own}).wait_send()

    count = len(pieces)

    def stage(p):
        events = [functools.partial(own, p + 2)] if p + 2 < count else []
        for k in range(depth):
            events.append(functools.partial(over, p, k))
            if p + 1 < count and k + 1 < depth:
                events.append(functools.partial(along, p + 1, k + 1))
        return events

    def run(events):
        for event in events:
            event()

    def slots(step, steps, slot, per, events):
        for i in range(steps):
            chosen = events[(i * per + slot) * len(events) // (steps * per) : (i * per + slot + 1) * len(events) // (steps * per)]
            if chosen:
                pl.when(step == i)(functools.partial(run, chosen))

    def pair_copy(i, src, dst):
        return pltpu.make_async_remote_copy(
            src_ref=src, dst_ref=dst, send_sem=pair_send.at[i], recv_sem=pair_recv.at[i],
            device_id={"tp": 1 - tp}, device_id_type=MESH,
        )

    def normalize(mine, gain):
        def chunk(i, carry):
            rows = pl.ds(pl.multiple_of(i * 128, 128), 128)
            a = mine[rows, :].astype(jnp.float32)
            b = peer[rows, :].astype(jnp.float32)
            total = jnp.sum(a * a, axis=-1, keepdims=True) + jnp.sum(b * b, axis=-1, keepdims=True)
            scale = lax.rsqrt(total / (2 * share) + EPS)
            here = pl.ds(pl.multiple_of(tp * share, LANES), share)
            there = pl.ds(pl.multiple_of((1 - tp) * share, LANES), share)
            normed[rows, here] = (a * scale * gain[:, here]).astype(jnp.bfloat16)
            normed[rows, there] = (b * scale * gain[:, there]).astype(jnp.bfloat16)
            return carry

        lax.fori_loop(0, length // 128, chunk, 0)

    def project(left, right):
        return jnp.dot(left, right, preferred_element_type=jnp.float32).astype(jnp.bfloat16)

    def mix(j, events, steps):
        cols = pl.ds(pl.multiple_of(j * LANES, LANES), LANES)
        hd = rate_ref.shape[1]
        slots(j, steps, 0, 3, events)
        linear = project(normed[...], w_lin[:, cols]).astype(jnp.float32)
        kernel_len = taps_ref.shape[0]
        filtered = linear * taps_ref[kernel_len - 1 : kernel_len, cols]
        for d in range(1, kernel_len):
            filtered = filtered + shift_rows(linear, d, 0.0) * taps_ref[kernel_len - 1 - d : kernel_len - d, cols]
        narrow = filtered.astype(jnp.bfloat16)
        for i in range(LANES // hd):
            part = slice(i * hd, (i + 1) * hd)
            lanes = pl.ds(pl.multiple_of(j * LANES + i * hd, hd), hd)
            block = j * (LANES // hd) + i
            piece = narrow[:, part]
            rate = jax.nn.sigmoid(jnp.dot(piece, rate_ref[block], preferred_element_type=jnp.float32))
            admit = jax.nn.sigmoid(jnp.dot(piece, admit_ref[block], preferred_element_type=jnp.float32))
            logit = logit_ref[:, lanes]
            slope = -GATE_SCALE * (jnp.maximum(-logit, 0.0) + jnp.log1p(jnp.exp(-jnp.abs(logit))))
            log_decay = rate * slope
            u = 2.0 * log_decay
            a = jnp.exp(log_decay)
            poly = 1.0 + u * (1.0 / 7.0)
            for c in (6.0, 5.0, 4.0, 3.0, 2.0):
                poly = 1.0 + u * (1.0 / c) * poly
            loss = jnp.where(u > -0.35, -u * poly, 1.0 - a * a)
            b = jnp.sqrt(loss) * admit * filtered[:, part]
            sub = lax.broadcasted_iota(jnp.int32, a.shape, 0) % 8
            for d in (1, 2, 4):
                keep = sub >= d
                pa = jnp.where(keep, pltpu.roll(a, d, 0), 1.0)
                pb = jnp.where(keep, pltpu.roll(b, d, 0), 0.0)
                b = a * pb + b
                a = a * pa
            a_ref[:, part] = a
            b_ref[:, part] = b
        slots(j, steps, 1, 3, events)

        def advance(t, carry):
            rows = pl.ds(pl.multiple_of(t * 8, 8), 8)
            s = a_ref[rows, :] * carry + b_ref[rows, :]
            b_ref[rows, :] = s
            return s[7:8, :]

        lax.fori_loop(0, length // 8, advance, jnp.zeros((1, LANES), jnp.float32), unroll=8)
        slots(j, steps, 2, 3, events)
        branch = project(normed[...], w_br[:, cols])
        for i in range(LANES // hd):
            part = slice(i * hd, (i + 1) * hd)
            lanes = pl.ds(pl.multiple_of(j * LANES + i * hd, hd), hd)
            gated = b_ref[:, part] * jax.nn.gelu(branch[:, part].astype(jnp.float32))
            scale = lax.rsqrt(jnp.mean(gated * gated, axis=-1, keepdims=True) + EPS)
            mixed[:, lanes] = (gated * scale * mix_out_gain[:, lanes]).astype(mixed.dtype)

    def feed(col, width):
        cols = pl.ds(col, width)

        def conv(weight, taps):
            v = project(normed[...], weight[:, cols]).astype(jnp.float32)
            n = taps.shape[0]
            out = v * taps[n - 1 : n, cols]
            for d in range(1, n):
                out = out + shift_rows(v, d, 0.0) * taps[n - 1 - d : n - d, cols]
            return out

        hidden[:, cols] = (jax.nn.silu(conv(w_gate, gtap_ref)) * conv(w_up, utap_ref)).astype(hidden.dtype)

    per = kept.shape[0]

    def share_out(f, left, weight, send, recv):
        result = project(left[...], weight[f])
        slot = f % per

        @pl.when(f // per == tp)
        def _():
            kept[slot] = result

        @pl.when(f // per != tp)
        def _():
            sent[slot] = result
            part_copy(slot, send, recv).start()

    def part_copy(slot, send, recv):
        return pltpu.make_async_remote_copy(
            src_ref=sent.at[slot], dst_ref=got.at[slot], send_sem=send.at[slot], recv_sem=recv.at[slot],
            device_id={"tp": 1 - tp}, device_id_type=MESH,
        )

    def add_up(base, target, send, recv):
        for i in range(per):
            cols = slice(i * LANES, (i + 1) * LANES)
            part_copy(i, send, recv).wait_recv()
            total = kept[i].astype(jnp.float32) + got[i].astype(jnp.float32)
            target[:, cols] = (base[:, cols].astype(jnp.float32) + total).astype(target.dtype)
        for i in range(per):
            part_copy(i, send, recv).wait_send()

    for m in range(6):
        own_copy(m).start()
    barrier = pltpu.get_barrier_semaphore()
    for device in ({"rep": 1 - x}, {"fs": line(z, 1 - y)}, {"tp": 1 - tp}):
        pl.semaphore_signal(barrier, inc=1, device_id=device, device_id_type=MESH)

    @pl.when(z > 0)
    def _():
        pl.semaphore_signal(barrier, inc=1, device_id={"fs": line(z - 1, y)}, device_id_type=MESH)

    @pl.when(z < depth - 1)
    def _():
        pl.semaphore_signal(barrier, inc=1, device_id={"fs": line(z + 1, y)}, device_id_type=MESH)

    pl.semaphore_wait(barrier, 3 + jnp.where(z > 0, 1, 0) + jnp.where(z < depth - 1, 1, 0))

    own(0)
    own(1)
    pair_copy(0, x_ref, peer).start()
    along(0, 1)
    pair_copy(0, x_ref, peer).wait()
    normalize(x_ref, mix_gain)
    for k in range(2, depth):
        along(0, k)
    bounds = (0,) + tuple(min(c, count) for c in CUTS) + (count,)
    early, mixing, summing, settling, waiting, ending = [
        [e for p in range(lo, hi) for e in stage(p)] for lo, hi in zip(bounds, bounds[1:])
    ]
    run(early)
    complete(0)
    complete(1)
    steps = share // LANES
    pl.loop(0, steps)(lambda j: mix(j, mixing, steps))
    complete(2)

    @pl.loop(0, 2 * per)
    def _(f):
        slots(f, 2 * per, 0, 1, summing)
        share_out(f, mixed, w_out, sum_send, sum_recv)

    add_up(x_ref, middle, sum_send, sum_recv)
    pair_copy(1, middle, peer).start()
    run(settling[: len(settling) // 2])
    pair_copy(1, middle, peer).wait()
    normalize(middle, ffn_gain)
    run(settling[len(settling) // 2 :])
    run(waiting)
    complete(3)
    complete(4)
    units = hidden.shape[1]
    wide = units // LANES
    first = len(ending) * wide // (wide + 1) if units % LANES else len(ending)

    @pl.loop(0, wide)
    def _(j):
        slots(j, wide, 0, 1, ending[:first])
        feed(pl.multiple_of(j * LANES, LANES), LANES)

    run(ending[first:])
    if units % LANES:
        feed(wide * LANES, units % LANES)

    @pl.loop(0, 2 * depth)
    def _(t):
        for k in range(depth):
            for side, waits in enumerate((landed, landed_across)):
                @pl.when(t == 2 * k + side)
                def _():
                    for p, piece in enumerate(pieces):
                        if piece[0] == 5:
                            waits(p, k)
        s = choose([order[i][0] for i in range(depth)], z)
        for k in range(1, depth):
            s = jnp.where(t // 2 == k, near(k), s)
        f = jnp.where(t % 2 == 0, line(s, y), line(s, 1 - y))
        share_out(f, hidden, w_down, end_send, end_recv)

    add_up(middle, o_ref, end_send, end_recv)
    for p in range(count):
        drain(p)


def fused(depth, stream_in, mix_gain, lin_weight, branch_weight, lin_taps, rate_blocks, admit_blocks, decay_logit,
          mix_out_gain, out_weight, ffn_gain, gate_weight, up_weight, gate_taps, up_taps, down_weight):
    own = stream_in[0]
    length, share = own.shape
    n = LINE * depth
    shards = (lin_weight, branch_weight, out_weight, gate_weight, up_weight, down_weight)
    pieces = plan(shards)
    bf = jnp.bfloat16
    whole = [
        pltpu.VMEM((n,) + w.shape, bf) if m in (2, 5) else pltpu.VMEM((n * w.shape[0], w.shape[1]), bf)
        for m, w in enumerate(shards)
    ]
    units = gate_weight.shape[1]
    channels = lin_weight.shape[1]
    width = out_weight.shape[1]
    count = len(pieces)
    dma = pltpu.SemaphoreType.DMA
    scratch = whole + [
        pltpu.VMEM((length, share), bf),
        pltpu.VMEM((length, 2 * share), bf),
        pltpu.VMEM((length, channels), bf),
        pltpu.VMEM((n // 2, length, width), bf),
        pltpu.VMEM((n // 2, length, width), bf),
        pltpu.VMEM((n // 2, length, width), bf),
        pltpu.VMEM((length, share), bf),
        pltpu.VMEM((length, units), bf),
        pltpu.VMEM((length, LANES), jnp.float32),
        pltpu.VMEM((length, LANES), jnp.float32),
        dma((6,)),
        dma((count, depth)),
        dma((count,)),
        dma((count, depth)),
        dma((count, depth)),
        dma((count, depth)),
        dma((count, depth)),
        dma((count, depth)),
        dma((count, depth)),
        dma((count, depth)),
        dma((2,)),
        dma((2,)),
        dma((n // 2,)),
        dma((n // 2,)),
        dma((n // 2,)),
        dma((n // 2,)),
    ]
    near = pl.BlockSpec(memory_space=pltpu.VMEM)
    far = pl.BlockSpec(memory_space=pl.ANY)
    macs = length * share * 2 * (3 * share + 3 * units)
    result = pl.pallas_call(
        functools.partial(layer_body, depth, pieces),
        in_specs=[near, near, far, far, near, near, near, near, near, far, near, far, far, near, near, far],
        out_specs=near,
        out_shape=jax.ShapeDtypeStruct((length, share), bf),
        scratch_shapes=scratch,
        compiler_params=pltpu.CompilerParams(collective_id=0, has_side_effects=True, vmem_limit_bytes=67043328),
        cost_estimate=pl.CostEstimate(flops=2 * macs, bytes_accessed=2 * macs // length, transcendentals=0),
        name="layer",
    )(own, mix_gain.reshape(1, -1), lin_weight, branch_weight, lin_taps, rate_blocks, admit_blocks, decay_logit.reshape(1, -1),
      mix_out_gain.reshape(1, -1), out_weight, ffn_gain.reshape(1, -1), gate_weight, up_weight, gate_taps,
      up_taps, down_weight)
    return result[None]


def gathered(tps, stream_in, mix_gain, lin_weight, branch_weight, lin_taps, rate_blocks, admit_blocks,
             decay_logit, mix_out_gain, out_weight, ffn_gain, gate_weight, up_weight, gate_taps, up_taps, down_weight):
    own = stream_in[0]
    length, share = own.shape

    def normed_rows(mine, gain):
        pair = lax.all_gather(mine, "tp", axis=0).astype(jnp.float32)
        mean_sq = jnp.sum(pair * pair, axis=(0, 2), keepdims=True) / (tps * share)
        y = (pair * lax.rsqrt(mean_sq + EPS) * gain.reshape(tps, 1, share)).astype(jnp.bfloat16)
        return y.transpose(1, 0, 2).reshape(length, tps * share)

    def product(left, right):
        return jnp.dot(left, right, preferred_element_type=jnp.float32).astype(jnp.bfloat16)

    def scatter(left, right):
        stack = product(left, right).reshape(length, tps, share).transpose(1, 0, 2)
        if tps == 2:
            tp = lax.axis_index("tp")
            mine = lax.dynamic_index_in_dim(stack, tp, 0, keepdims=False)
            other = lax.dynamic_index_in_dim(stack, 1 - tp, 0, keepdims=False)
            other = lax.ppermute(other, "tp", [(0, 1), (1, 0)])
            return mine.astype(jnp.float32) + other.astype(jnp.float32)
        return lax.psum_scatter(stack, "tp", scatter_dimension=0, tiled=False).astype(jnp.float32)

    def gather(w, axis=0):
        return lax.all_gather(w, "fs", axis=axis, tiled=True)

    normed = normed_rows(own, mix_gain)
    linear = product(normed, gather(lin_weight))
    branch = product(normed, gather(branch_weight))
    slope = (-GATE_SCALE * jax.nn.softplus(-decay_logit)).reshape(1, -1)
    mixed = mixer(linear, branch, lin_taps, rate_blocks, admit_blocks, slope, mix_out_gain.reshape(1, -1))
    middle = (own.astype(jnp.float32) + scatter(mixed, gather(out_weight, 1))).astype(jnp.bfloat16)
    normed2 = normed_rows(middle, ffn_gain)
    gate_pre = product(normed2, gather(gate_weight))
    up_pre = product(normed2, gather(up_weight))
    hidden = ffn_gate(gate_pre, up_pre, gate_taps, up_taps)
    result = (middle.astype(jnp.float32) + scatter(hidden, gather(down_weight, 1))).astype(jnp.bfloat16)
    return result[None]


def solution(mesh):
    placed = (
        P(("rep", "fs"), None, "tp"),
        P(),
        P("fs", "tp"),
        P("fs", "tp"),
        P(None, "tp"),
        P("tp", None, None),
        P("tp", None, None),
        P("tp"),
        P("tp"),
        P("tp", "fs"),
        P(),
        P("fs", "tp"),
        P("fs", "tp"),
        P(None, "tp"),
        P(None, "tp"),
        P("tp", "fs"),
    )
    reps, n, tps = mesh.shape["rep"], mesh.shape["fs"], mesh.shape["tp"]
    if reps == 2 and tps == 2 and n == 8:
        body = functools.partial(fused, n // LINE)
    else:
        body = functools.partial(gathered, tps)
    return jax.shard_map(
        body, mesh=mesh, in_specs=placed, out_specs=P(("rep", "fs"), None, "tp"), check_vma=False
    )
```

```python
import functools

import jax
import jax.numpy as jnp
from jax import lax
from jax.experimental import pallas as pl
from jax.experimental.pallas import tpu as pltpu
from jax.sharding import PartitionSpec as P

EPS = 1e-06
GATE_SCALE = 8.0
MESH = pl.DeviceIdType.MESH
LANES = 256
LINE = 2


def shift_rows(x, d, fill):
    rows = lax.broadcasted_iota(jnp.int32, x.shape, 0)
    return jnp.where(rows < d, fill, pltpu.roll(x, d, 0))


def mixer_body(lin_ref, br_ref, taps_ref, rate_ref, admit_ref, slope_ref, gain_ref, o_ref, a_ref, b_ref):
    length, width = lin_ref.shape
    hd = rate_ref.shape[1]
    linear = lin_ref[...].astype(jnp.float32)
    kernel_len = taps_ref.shape[0]
    filtered = linear * taps_ref[kernel_len - 1 : kernel_len]
    for d in range(1, kernel_len):
        filtered = filtered + shift_rows(linear, d, 0.0) * taps_ref[kernel_len - 1 - d : kernel_len - d]
    narrow = filtered.astype(jnp.bfloat16)
    for j in range(width // hd):
        cols = slice(j * hd, (j + 1) * hd)
        piece = narrow[:, cols]
        rate = jax.nn.sigmoid(jnp.dot(piece, rate_ref[j], preferred_element_type=jnp.float32))
        admit = jax.nn.sigmoid(jnp.dot(piece, admit_ref[j], preferred_element_type=jnp.float32))
        log_decay = rate * slope_ref[:, cols]
        u = 2.0 * log_decay
        decay = jnp.exp(log_decay)
        poly = 1.0 + u * (1.0 / 7.0)
        for c in (6.0, 5.0, 4.0, 3.0, 2.0):
            poly = 1.0 + u * (1.0 / c) * poly
        loss = jnp.where(u > -0.35, -u * poly, 1.0 - decay * decay)
        a = decay
        b = jnp.sqrt(loss) * admit * filtered[:, cols]
        sub = lax.broadcasted_iota(jnp.int32, a.shape, 0) % 8
        for d in (1, 2, 4):
            keep = sub >= d
            pa = jnp.where(keep, pltpu.roll(a, d, 0), 1.0)
            pb = jnp.where(keep, pltpu.roll(b, d, 0), 0.0)
            b = a * pb + b
            a = a * pa
        a_ref[:, cols] = a
        b_ref[:, cols] = b

    def advance(t, carry):
        rows = pl.ds(pl.multiple_of(t * 8, 8), 8)
        s = a_ref[rows, :] * carry + b_ref[rows, :]
        b_ref[rows, :] = s
        return s[7:8, :]

    lax.fori_loop(0, length // 8, advance, jnp.zeros((1, width), jnp.float32), unroll=8)
    for j in range(width // hd):
        cols = slice(j * hd, (j + 1) * hd)
        gated = b_ref[:, cols] * jax.nn.gelu(br_ref[:, cols].astype(jnp.float32))
        scale = lax.rsqrt(jnp.mean(gated * gated, axis=-1, keepdims=True) + EPS)
        o_ref[:, cols] = (gated * scale * gain_ref[:, cols]).astype(o_ref.dtype)


def mixer(linear, branch, taps, rate_blocks, admit_blocks, slope, gain):
    length, channels = linear.shape
    hd = rate_blocks.shape[1]
    per = 2 if rate_blocks.shape[0] % 2 == 0 else 1
    width = per * hd
    wide = pl.BlockSpec((length, width), lambda i: (0, i))
    row = pl.BlockSpec((1, width), lambda i: (0, i))
    blk = pl.BlockSpec((per, hd, hd), lambda i: (i, 0, 0))
    return pl.pallas_call(
        mixer_body,
        grid=(channels // width,),
        in_specs=[wide, wide, pl.BlockSpec((taps.shape[0], width), lambda i: (0, i)), blk, blk, row, row],
        out_specs=wide,
        out_shape=jax.ShapeDtypeStruct((length, channels), jnp.bfloat16),
        scratch_shapes=[pltpu.VMEM((length, width), jnp.float32), pltpu.VMEM((length, width), jnp.float32)],
        cost_estimate=pl.CostEstimate(flops=length * channels * 20000, bytes_accessed=length * channels * 6, transcendentals=0),
        name="mixer",
    )(linear, branch, taps, rate_blocks, admit_blocks, slope, gain)


def ffn_body(g_ref, u_ref, gt_ref, ut_ref, o_ref):
    def conv(ref, taps):
        x = ref[...].astype(jnp.float32)
        n = taps.shape[0]
        y = x * taps[n - 1 : n]
        for d in range(1, n):
            y = y + shift_rows(x, d, 0.0) * taps[n - 1 - d : n - d]
        return y

    o_ref[...] = (jax.nn.silu(conv(g_ref, gt_ref)) * conv(u_ref, ut_ref)).astype(o_ref.dtype)


def ffn_gate(gate_pre, up_pre, gate_taps, up_taps):
    length, units = gate_pre.shape
    width = 128
    wide = pl.BlockSpec((length, width), lambda i: (0, i))
    tap = pl.BlockSpec((gate_taps.shape[0], width), lambda i: (0, i))
    return pl.pallas_call(
        ffn_body,
        grid=(units // width,),
        in_specs=[wide, wide, tap, tap],
        out_specs=wide,
        out_shape=jax.ShapeDtypeStruct((length, units), jnp.bfloat16),
        cost_estimate=pl.CostEstimate(flops=length * units * 8000, bytes_accessed=length * units * 6, transcendentals=0),
        name="ffn_gate",
    )(gate_pre, up_pre, gate_taps, up_taps)


SPLIT = (
    ((8, 8,), (8, 8,),),
    ((8, 8,), (8, 8,),),
    ((8, 8,),),
    ((4, 4,), (8, 8,),),
    ((4, 4,), (8, 4,),),
    ((6, 6,), (8, 4,), (8, 4,), (8, 4,),),
)
OPENING = (
    ((0, 0, 0,), (0, 5, 0,), (0, 3, 0,), (0, 1, 0,), (0, 2, 0,), (1, 3, 1,), (0, 6, 0,), (1, 0, 1,),),
    ((1, 1, 1,), (1, 0, 2,), (1, 3, 2,), (1, 5, 1,), (1, 5, 2,),),
    ((1, 3, 3,), (1, 0, 3,), (0, 4, 0,), (1, 2, 1,), (1, 1, 2,), (1, 2, 2,), (2, 6, 0,), (2, 0, 0,), (2, 5, 0,), (1, 1, 3,), (1, 2, 3,),),
    ((2, 1, 1,), (2, 5, 2,), (1, 4, 2,), (1, 4, 1,), (2, 2, 0,), (1, 4, 3,),),
    ((2, 3, 0,), (1, 6, 2,), (1, 6, 1,), (2, 4, 0,), (2, 2, 1,), (2, 0, 1,), (2, 1, 2,), (2, 0, 3,), (2, 2, 2,), (2, 3, 1,), (1, 5, 3,), (2, 3, 2,), (2, 0, 2,), (0, 11, 0,), (0, 8, 0,), (2, 1, 3,), (2, 2, 3,), (2, 3, 3,), (2, 1, 0,),),
    ((2, 4, 2,), (2, 6, 2,), (1, 11, 1,),),
)
MIXING = (
    ((), ((2, 5, 1,),), (), ((2, 8, 1,),),),
    ((), (), ((2, 5, 3,), (1, 8, 2,),), ((2, 8, 0,), (1, 7, 2,),),),
    ((), ((1, 6, 3,), (1, 8, 1,), (0, 10, 0,), (0, 7, 0,), (2, 4, 1,), (2, 4, 3,),), ((1, 8, 3,),), ((1, 7, 1,), (1, 7, 3,), (1, 10, 1,),),),
)
SUMMING = (
    (),
    ((0, 12, 0,),),
    (),
    (),
    (),
    (),
    ((2, 6, 1,),),
    (),
    (),
    (),
    (),
    (),
    ((1, 10, 2,),),
    (),
    (),
    ((2, 6, 3,), (2, 7, 0,), (1, 11, 2,), (2, 8, 3,), (2, 8, 2,), (2, 10, 0,), (2, 11, 1,),),
)
SETTLING = (
    ((2, 12, 0,), (1, 12, 1,), (0, 9, 0,),),
    ((2, 11, 0,), (1, 12, 2,), (2, 7, 2,),),
    ((1, 10, 3,), (1, 11, 3,), (1, 9, 1,), (2, 7, 3,), (2, 7, 1,),),
)
ENDING = (
    (),
    ((2, 10, 2,), (1, 9, 2,),),
    ((2, 11, 2,), (2, 12, 1,), (1, 12, 3,),),
    ((2, 10, 1,), (1, 9, 3,), (2, 11, 3,),),
    ((2, 9, 1,), (2, 10, 3,), (2, 9, 0,), (2, 12, 2,),),
    ((2, 9, 2,),),
    ((2, 12, 3,), (2, 9, 3,),),
)


def plan(heights):
    cuts = []
    for m, rows in enumerate(heights):
        parts = len(SPLIT[m])
        step = -(-rows // (128 * parts)) * 128
        cuts.append([(m, at, min(step, rows - at)) + SPLIT[m][i] for i, at in enumerate(range(0, rows, step))])
    pieces = []
    for group in ((0, 1), (2,), (3, 4), (5,)):
        for i in range(max(len(cuts[m]) for m in group)):
            pieces += [cuts[m][i] for m in group if i < len(cuts[m])]
    return pieces


def nearest(depth):
    return [sorted(range(depth), key=lambda s: (abs(s - z), -s)) for z in range(depth)]


def choose(values, at):
    out = jnp.int32(values[0])
    for i, v in enumerate(values[1:], 1):
        out = jnp.where(at == i, jnp.int32(v), out)
    return out


def layer_body(depth, pieces, x_ref, mix_gain, lin_hbm, br_hbm, taps_ref, rate_ref, admit_ref, logit_ref,
               mix_out_gain, out_hbm, ffn_gain, gate_hbm, up_hbm, gtap_ref, utap_ref, down_hbm, o_ref,
               w_lin, w_br, w_out, w_gate, w_up, w_down, peer, normed, mixed, kept, sent, got, middle, hidden,
               a_ref, b_ref, visit, toward, inward, local_sem, z_send, z_extra, z_recv, y_send, y_recv, p_send, p_recv, q_send, q_recv,
               pair_send, pair_recv, sum_send, sum_recv, end_send, end_recv, visit_send, visit_recv, part_send, part_recv):
    x = lax.axis_index("rep")
    f_own = lax.axis_index("fs")
    tp = lax.axis_index("tp")
    z, y = f_own // LINE, f_own % LINE
    length, share = x_ref.shape
    order = nearest(depth)
    hbm = (lin_hbm, br_hbm, out_hbm, gate_hbm, up_hbm, down_hbm)
    full = (w_lin, w_br, w_out, w_gate, w_up, w_down)
    flat = tuple(len(w.shape) == 2 for w in full)
    height = tuple(w.shape[0] // (LINE * depth) if flat[m] else w.shape[1] for m, w in enumerate(full))
    half = w_lin.shape[1]

    def line(s, row):
        return s * LINE + row

    def near(k):
        return choose([order[i][k] for i in range(depth)], z)

    def view(p, f, start, size):
        m, row0 = pieces[p][:2]
        start = pl.multiple_of(row0 + start, 16)
        if flat[m]:
            return full[m].at[pl.ds(pl.multiple_of(f * height[m] + start, 16), size), :]
        return full[m].at[f, pl.ds(start, size), :]

    def parts(p):
        q, (u, v) = pieces[p][2] // 8, pieces[p][3:]
        return {
            "z": ((8 - u) * q * x, u * q),
            "y": ((8 - v) * q * x, v * q),
            "p_out": (u * q * x, (8 - u) * q),
            "p_in": (u * q * (1 - x), (8 - u) * q),
            "q_out": (v * q * x, (8 - v) * q),
            "q_in": (v * q * (1 - x), (8 - v) * q),
        }

    def spare(p, side):
        return pieces[p][3 + side] < 8

    def push(p, f, part, send, recv, device):
        ref = view(p, f, *parts(p)[part])
        return pltpu.make_async_remote_copy(
            src_ref=ref, dst_ref=ref, send_sem=send, recv_sem=recv, device_id=device, device_id_type=MESH
        )

    def own_copy(m):
        src = hbm[m]
        if m < 2:
            src = src.at[:, pl.ds(pl.multiple_of(x * half, LANES), half)]
        if m == 2:
            src = src.at[pl.ds(pl.multiple_of(x * half, LANES), half), :]
        dst = full[m].at[pl.ds(pl.multiple_of(f_own * height[m], 16), height[m]), :] if flat[m] else full[m].at[f_own]
        return pltpu.make_async_copy(src, dst, local_sem.at[m])

    def own(p):
        @pl.when(z < depth - 1)
        def _():
            push(p, f_own, "z", z_send.at[p, z], z_recv.at[p, z], {"fs": line(z + 1, y)}).start()

        @pl.when(z > 0)
        def _():
            push(p, f_own, "z", z_extra.at[p], z_recv.at[p, z], {"fs": line(z - 1, y)}).start()

        push(p, f_own, "y", y_send.at[p, z], y_recv.at[p, z], {"fs": line(z, 1 - y)}).start()

    def along(p, k):
        s = near(k)
        f = line(s, y)
        push(p, f, "z", z_send.at[p, s], z_recv.at[p, s], {"fs": f_own}).wait_recv()
        onward = jnp.where(s < z, z + 1, z - 1)

        @pl.when(jnp.logical_and(onward >= 0, onward < depth))
        def _():
            push(p, f, "z", z_send.at[p, s], z_recv.at[p, s], {"fs": line(onward, y)}).start()

        push(p, f, "y", y_send.at[p, s], y_recv.at[p, s], {"fs": line(z, 1 - y)}).start()
        if spare(p, 0):
            push(p, f, "p_out", p_send.at[p, s], p_recv.at[p, s], {"rep": 1 - x}).start()

    def over(p, k):
        s = near(k)
        f = line(s, 1 - y)
        push(p, f, "y", y_send.at[p, s], y_recv.at[p, s], {"fs": f_own}).wait_recv()
        if spare(p, 1):
            push(p, f, "q_out", q_send.at[p, s], q_recv.at[p, s], {"rep": 1 - x}).start()

    def landed(p, k):
        s = near(k)
        if k and spare(p, 0):
            push(p, line(s, y), "p_in", p_send.at[p, s], p_recv.at[p, s], {"rep": 1 - x}).wait_recv()

    def landed_across(p, k):
        s = near(k)
        if spare(p, 1):
            push(p, line(s, 1 - y), "q_in", q_send.at[p, s], q_recv.at[p, s], {"rep": 1 - x}).wait_recv()

    def complete(m):
        for p, piece in enumerate(pieces):
            if piece[0] == m:
                for k in range(depth):
                    landed(p, k)
                    landed_across(p, k)

    def drain(p):
        @pl.when(z < depth - 1)
        def _():
            push(p, f_own, "z", z_send.at[p, z], z_recv.at[p, z], {"fs": f_own}).wait_send()

        @pl.when(z > 0)
        def _():
            push(p, f_own, "z", z_extra.at[p], z_recv.at[p, z], {"fs": f_own}).wait_send()

        for k in range(depth):
            s = near(k)
            f = line(s, y)
            push(p, f, "y", y_send.at[p, s], y_recv.at[p, s], {"fs": f_own}).wait_send()
            if spare(p, 1):
                push(p, line(s, 1 - y), "q_out", q_send.at[p, s], q_recv.at[p, s], {"fs": f_own}).wait_send()
            if k:
                if spare(p, 0):
                    push(p, f, "p_out", p_send.at[p, s], p_recv.at[p, s], {"fs": f_own}).wait_send()
                onward = jnp.where(s < z, z + 1, z - 1)

                @pl.when(jnp.logical_and(onward >= 0, onward < depth))
                def _():
                    push(p, f, "z", z_send.at[p, s], z_recv.at[p, s], {"fs": f_own}).wait_send()

    count = len(pieces)

    def run(events):
        for kind, p, k in events:
            if kind == 0:
                own(p)
            elif kind == 1:
                along(p, k)
            else:
                over(p, k)

    def slots(step, groups):
        for i, events in enumerate(groups):
            if events:
                pl.when(step == i)(functools.partial(run, events))

    def pair_copy(i, src, dst):
        return pltpu.make_async_remote_copy(
            src_ref=src, dst_ref=dst, send_sem=pair_send.at[i], recv_sem=pair_recv.at[i],
            device_id={"tp": 1 - tp}, device_id_type=MESH,
        )

    def normalize(mine, theirs, gain, target):
        def chunk(i, carry):
            rows = pl.ds(pl.multiple_of(i * 128, 128), 128)
            a = mine[rows, :].astype(jnp.float32)
            b = theirs[rows, :].astype(jnp.float32)
            total = jnp.sum(a * a, axis=-1, keepdims=True) + jnp.sum(b * b, axis=-1, keepdims=True)
            scale = lax.rsqrt(total / (2 * share) + EPS)
            here = pl.ds(pl.multiple_of(tp * share, LANES), share)
            there = pl.ds(pl.multiple_of((1 - tp) * share, LANES), share)
            target[rows, here] = (a * scale * gain[:, here]).astype(jnp.bfloat16)
            target[rows, there] = (b * scale * gain[:, there]).astype(jnp.bfloat16)
            return carry

        lax.fori_loop(0, length // 128, chunk, 0)

    def project(left, right):
        return jnp.dot(left, right, preferred_element_type=jnp.float32).astype(jnp.bfloat16)

    tiles = half // LANES

    def mix(s, j):
        cols = pl.ds(pl.multiple_of(j * LANES, LANES), LANES)
        wide = pl.ds(pl.multiple_of(x * half + j * LANES, LANES), LANES)
        hd = rate_ref.shape[1]
        step = s * tiles + j
        slots(step, MIXING[0])
        linear = project(normed[s], w_lin[:, cols]).astype(jnp.float32)
        kernel_len = taps_ref.shape[0]
        filtered = linear * taps_ref[kernel_len - 1 : kernel_len, wide]
        for d in range(1, kernel_len):
            filtered = filtered + shift_rows(linear, d, 0.0) * taps_ref[kernel_len - 1 - d : kernel_len - d, wide]
        narrow = filtered.astype(jnp.bfloat16)
        for i in range(LANES // hd):
            part = slice(i * hd, (i + 1) * hd)
            lanes = pl.ds(pl.multiple_of(x * half + j * LANES + i * hd, hd), hd)
            block = x * (half // hd) + j * (LANES // hd) + i
            piece = narrow[:, part]
            rate = jax.nn.sigmoid(jnp.dot(piece, rate_ref[block], preferred_element_type=jnp.float32))
            admit = jax.nn.sigmoid(jnp.dot(piece, admit_ref[block], preferred_element_type=jnp.float32))
            logit = logit_ref[:, lanes]
            slope = -GATE_SCALE * (jnp.maximum(-logit, 0.0) + jnp.log1p(jnp.exp(-jnp.abs(logit))))
            log_decay = rate * slope
            u = 2.0 * log_decay
            a = jnp.exp(log_decay)
            poly = 1.0 + u * (1.0 / 7.0)
            for c in (6.0, 5.0, 4.0, 3.0, 2.0):
                poly = 1.0 + u * (1.0 / c) * poly
            loss = jnp.where(u > -0.35, -u * poly, 1.0 - a * a)
            b = jnp.sqrt(loss) * admit * filtered[:, part]
            sub = lax.broadcasted_iota(jnp.int32, a.shape, 0) % 8
            for d in (1, 2, 4):
                keep = sub >= d
                pa = jnp.where(keep, pltpu.roll(a, d, 0), 1.0)
                pb = jnp.where(keep, pltpu.roll(b, d, 0), 0.0)
                b = a * pb + b
                a = a * pa
            a_ref[:, part] = a
            b_ref[:, part] = b
        slots(step, MIXING[1])

        def advance(t, carry):
            rows = pl.ds(pl.multiple_of(t * 8, 8), 8)
            s = a_ref[rows, :] * carry + b_ref[rows, :]
            b_ref[rows, :] = s
            return s[7:8, :]

        lax.fori_loop(0, length // 8, advance, jnp.zeros((1, LANES), jnp.float32), unroll=8)
        slots(step, MIXING[2])
        branch = project(normed[s], w_br[:, cols])
        for i in range(LANES // hd):
            part = slice(i * hd, (i + 1) * hd)
            lanes = pl.ds(pl.multiple_of(x * half + j * LANES + i * hd, hd), hd)
            local = pl.ds(pl.multiple_of(j * LANES + i * hd, hd), hd)
            gated = b_ref[:, part] * jax.nn.gelu(branch[:, part].astype(jnp.float32))
            scale = lax.rsqrt(jnp.mean(gated * gated, axis=-1, keepdims=True) + EPS)
            mixed[:, local] = (gated * scale * mix_out_gain[:, lanes]).astype(mixed.dtype)

    def feed(col, width):
        cols = pl.ds(col, width)

        def conv(weight, taps):
            v = project(normed[0], weight[:, cols]).astype(jnp.float32)
            n = taps.shape[0]
            out = v * taps[n - 1 : n, cols]
            for d in range(1, n):
                out = out + shift_rows(v, d, 0.0) * taps[n - 1 - d : n - d, cols]
            return out

        hidden[:, cols] = (jax.nn.silu(conv(w_gate, gtap_ref)) * conv(w_up, utap_ref)).astype(hidden.dtype)

    per = kept.shape[0]

    def share_out(f, left, weight, s, send, recv):
        result = project(left[...], weight[f])
        slot = f % per

        @pl.when(f // per == tp)
        def _():
            kept[slot] = result

        @pl.when(f // per != tp)
        def _():
            sent[slot] = result
            part_copy(slot, s, send, recv).start()

    def part_copy(slot, s, send, recv):
        return pltpu.make_async_remote_copy(
            src_ref=sent.at[slot], dst_ref=got.at[s, slot], send_sem=send.at[s, slot], recv_sem=recv.at[s, slot],
            device_id={"tp": 1 - tp}, device_id_type=MESH,
        )

    def swap_copy(src, dst, send, recv):
        return pltpu.make_async_remote_copy(
            src_ref=src, dst_ref=dst, send_sem=send, recv_sem=recv, device_id={"rep": 1 - x}, device_id_type=MESH
        )

    def visit_copy():
        return swap_copy(x_ref, visit, visit_send, visit_recv)

    def toward_copy(i):
        return swap_copy(toward.at[i], inward.at[i], part_send.at[i], part_recv.at[i])

    def summed(i, s):
        return kept[i].astype(jnp.float32) + got[s, i].astype(jnp.float32)

    for m in range(6):
        own_copy(m).start()
    barrier = pltpu.get_barrier_semaphore()
    for device in ({"rep": 1 - x}, {"fs": line(z, 1 - y)}, {"tp": 1 - tp}):
        pl.semaphore_signal(barrier, inc=1, device_id=device, device_id_type=MESH)

    @pl.when(z > 0)
    def _():
        pl.semaphore_signal(barrier, inc=1, device_id={"fs": line(z - 1, y)}, device_id_type=MESH)

    @pl.when(z < depth - 1)
    def _():
        pl.semaphore_signal(barrier, inc=1, device_id={"fs": line(z + 1, y)}, device_id_type=MESH)

    pl.semaphore_wait(barrier, 3 + jnp.where(z > 0, 1, 0) + jnp.where(z < depth - 1, 1, 0))

    ready = []

    def prepare(events):
        for event in events:
            m = pieces[event[1]][0]
            if event[0] == 0 and m not in ready:
                own_copy(m).wait()
                ready.append(m)
            run((event,))

    prepare(OPENING[0])
    visit_copy().start()
    pair_copy(0, x_ref, peer.at[0]).start()
    prepare(OPENING[1])
    pair_copy(0, x_ref, peer.at[0]).wait()
    normalize(x_ref, peer.at[0], mix_gain, normed.at[1])
    prepare(OPENING[2])
    visit_copy().wait()
    pair_copy(1, visit, peer.at[1]).start()
    prepare(OPENING[3])
    pair_copy(1, visit, peer.at[1]).wait()
    normalize(visit, peer.at[1], mix_gain, normed.at[0])
    prepare(OPENING[4])
    for m in range(6):
        if m not in ready:
            own_copy(m).wait()
    complete(0)
    complete(1)

    @pl.loop(0, 2)
    def _(s):
        pl.loop(0, tiles)(lambda j: mix(s, j))

        @pl.when(s == 0)
        def _():
            run(OPENING[5])
            complete(2)

        @pl.loop(0, 2 * per)
        def _(f):
            slots(s * 2 * per + f, SUMMING)
            share_out(f, mixed, w_out, s, sum_send, sum_recv)

        for i in range(per):
            part_copy(i, s, sum_send, sum_recv).wait_send()
            part_copy(i, s, sum_send, sum_recv).wait_recv()

            @pl.when(s == 0)
            def _():
                toward[i] = summed(i, 0).astype(jnp.bfloat16)
                toward_copy(i).start()

    run(SETTLING[0])
    for i in range(per):
        cols = slice(i * LANES, (i + 1) * LANES)
        toward_copy(i).wait_recv()
        total = summed(i, 1) + inward[i].astype(jnp.float32)
        middle[:, cols] = (x_ref[:, cols].astype(jnp.float32) + total).astype(middle.dtype)
    pair_copy(2, middle, peer.at[0]).start()
    run(SETTLING[1])
    pair_copy(2, middle, peer.at[0]).wait()
    normalize(middle, peer.at[0], ffn_gain, normed.at[0])
    run(SETTLING[2])
    complete(3)
    complete(4)
    units = hidden.shape[1]
    wide = units // LANES

    @pl.loop(0, wide)
    def _(j):
        slots(j, ENDING[:wide])
        feed(pl.multiple_of(j * LANES, LANES), LANES)

    for events in ENDING[wide:-1]:
        run(events)
    if units % LANES:
        feed(wide * LANES, units % LANES)
    run(ENDING[-1])

    @pl.loop(0, 2 * depth)
    def _(t):
        for k in range(depth):
            for side, waits in enumerate((landed, landed_across)):
                @pl.when(t == 2 * k + side)
                def _():
                    for p, piece in enumerate(pieces):
                        if piece[0] == 5:
                            waits(p, k)
        s = choose([order[i][0] for i in range(depth)], z)
        for k in range(1, depth):
            s = jnp.where(t // 2 == k, near(k), s)
        f = jnp.where(t % 2 == 0, line(s, y), line(s, 1 - y))
        share_out(f, hidden, w_down, 0, end_send, end_recv)

    for i in range(per):
        cols = slice(i * LANES, (i + 1) * LANES)
        part_copy(i, 0, end_send, end_recv).wait_recv()
        o_ref[:, cols] = (middle[:, cols].astype(jnp.float32) + summed(i, 0)).astype(o_ref.dtype)
    for i in range(per):
        part_copy(i, 0, end_send, end_recv).wait_send()
        toward_copy(i).wait_send()
    for p in range(count):
        drain(p)


def fused(depth, stream_in, mix_gain, lin_weight, branch_weight, lin_taps, rate_blocks, admit_blocks, decay_logit,
          mix_out_gain, out_weight, ffn_gain, gate_weight, up_weight, gate_taps, up_taps, down_weight):
    own = stream_in[0]
    length, share = own.shape
    n = LINE * depth
    shards = (lin_weight, branch_weight, out_weight, gate_weight, up_weight, down_weight)
    half = lin_weight.shape[1] // 2
    heights = [half if m == 2 else w.shape[0] for m, w in enumerate(shards)]
    widths = [half if m < 2 else w.shape[1] for m, w in enumerate(shards)]
    pieces = plan(heights)
    bf = jnp.bfloat16
    whole = [
        pltpu.VMEM((n, h, w), bf) if m in (2, 5) else pltpu.VMEM((n * h, w), bf)
        for m, (h, w) in enumerate(zip(heights, widths))
    ]
    units = gate_weight.shape[1]
    width = out_weight.shape[1]
    count = len(pieces)
    dma = pltpu.SemaphoreType.DMA
    scratch = whole + [
        pltpu.VMEM((2, length, share), bf),
        pltpu.VMEM((2, length, 2 * share), bf),
        pltpu.VMEM((length, half), bf),
        pltpu.VMEM((n // 2, length, width), bf),
        pltpu.VMEM((n // 2, length, width), bf),
        pltpu.VMEM((2, n // 2, length, width), bf),
        pltpu.VMEM((length, share), bf),
        pltpu.VMEM((length, units), bf),
        pltpu.VMEM((length, LANES), jnp.float32),
        pltpu.VMEM((length, LANES), jnp.float32),
        pltpu.VMEM((length, share), bf),
        pltpu.VMEM((n // 2, length, width), bf),
        pltpu.VMEM((n // 2, length, width), bf),
        dma((6,)),
        dma((count, depth)),
        dma((count,)),
        dma((count, depth)),
        dma((count, depth)),
        dma((count, depth)),
        dma((count, depth)),
        dma((count, depth)),
        dma((count, depth)),
        dma((count, depth)),
        dma((3,)),
        dma((3,)),
        dma((2, n // 2)),
        dma((2, n // 2)),
        dma((1, n // 2)),
        dma((1, n // 2)),
        dma,
        dma,
        dma((n // 2,)),
        dma((n // 2,)),
    ]
    near = pl.BlockSpec(memory_space=pltpu.VMEM)
    far = pl.BlockSpec(memory_space=pl.ANY)
    macs = length * share * 2 * (3 * share + 3 * units)
    result = pl.pallas_call(
        functools.partial(layer_body, depth, pieces),
        in_specs=[near, near, far, far, near, near, near, near, near, far, near, far, far, near, near, far],
        out_specs=near,
        out_shape=jax.ShapeDtypeStruct((length, share), bf),
        scratch_shapes=scratch,
        compiler_params=pltpu.CompilerParams(collective_id=0, has_side_effects=True, vmem_limit_bytes=67043328),
        cost_estimate=pl.CostEstimate(flops=2 * macs, bytes_accessed=2 * macs // length, transcendentals=0),
        name="layer",
    )(own, mix_gain.reshape(1, -1), lin_weight, branch_weight, lin_taps, rate_blocks, admit_blocks, decay_logit.reshape(1, -1),
      mix_out_gain.reshape(1, -1), out_weight, ffn_gain.reshape(1, -1), gate_weight, up_weight, gate_taps,
      up_taps, down_weight)
    return result[None]


def gathered(tps, stream_in, mix_gain, lin_weight, branch_weight, lin_taps, rate_blocks, admit_blocks,
             decay_logit, mix_out_gain, out_weight, ffn_gain, gate_weight, up_weight, gate_taps, up_taps, down_weight):
    own = stream_in[0]
    length, share = own.shape

    def normed_rows(mine, gain):
        pair = lax.all_gather(mine, "tp", axis=0).astype(jnp.float32)
        mean_sq = jnp.sum(pair * pair, axis=(0, 2), keepdims=True) / (tps * share)
        y = (pair * lax.rsqrt(mean_sq + EPS) * gain.reshape(tps, 1, share)).astype(jnp.bfloat16)
        return y.transpose(1, 0, 2).reshape(length, tps * share)

    def product(left, right):
        return jnp.dot(left, right, preferred_element_type=jnp.float32).astype(jnp.bfloat16)

    def scatter(left, right):
        stack = product(left, right).reshape(length, tps, share).transpose(1, 0, 2)
        if tps == 2:
            tp = lax.axis_index("tp")
            mine = lax.dynamic_index_in_dim(stack, tp, 0, keepdims=False)
            other = lax.dynamic_index_in_dim(stack, 1 - tp, 0, keepdims=False)
            other = lax.ppermute(other, "tp", [(0, 1), (1, 0)])
            return mine.astype(jnp.float32) + other.astype(jnp.float32)
        return lax.psum_scatter(stack, "tp", scatter_dimension=0, tiled=False).astype(jnp.float32)

    def gather(w, axis=0):
        return lax.all_gather(w, "fs", axis=axis, tiled=True)

    normed = normed_rows(own, mix_gain)
    linear = product(normed, gather(lin_weight))
    branch = product(normed, gather(branch_weight))
    slope = (-GATE_SCALE * jax.nn.softplus(-decay_logit)).reshape(1, -1)
    mixed = mixer(linear, branch, lin_taps, rate_blocks, admit_blocks, slope, mix_out_gain.reshape(1, -1))
    middle = (own.astype(jnp.float32) + scatter(mixed, gather(out_weight, 1))).astype(jnp.bfloat16)
    normed2 = normed_rows(middle, ffn_gain)
    gate_pre = product(normed2, gather(gate_weight))
    up_pre = product(normed2, gather(up_weight))
    hidden = ffn_gate(gate_pre, up_pre, gate_taps, up_taps)
    result = (middle.astype(jnp.float32) + scatter(hidden, gather(down_weight, 1))).astype(jnp.bfloat16)
    return result[None]


def solution(mesh):
    placed = (
        P(("rep", "fs"), None, "tp"),
        P(),
        P("fs", "tp"),
        P("fs", "tp"),
        P(None, "tp"),
        P("tp", None, None),
        P("tp", None, None),
        P("tp"),
        P("tp"),
        P("tp", "fs"),
        P(),
        P("fs", "tp"),
        P("fs", "tp"),
        P(None, "tp"),
        P(None, "tp"),
        P("tp", "fs"),
    )
    reps, n, tps = mesh.shape["rep"], mesh.shape["fs"], mesh.shape["tp"]
    if reps == 2 and tps == 2 and n == 8:
        body = functools.partial(fused, n // LINE)
    else:
        body = functools.partial(gathered, tps)
    return jax.shard_map(
        body, mesh=mesh, in_specs=placed, out_specs=P(("rep", "fs"), None, "tp"), check_vma=False
    )
```

```python
import functools

import jax
import jax.numpy as jnp
from jax import lax
from jax.experimental import pallas as pl
from jax.experimental.pallas import tpu as pltpu
from jax.sharding import PartitionSpec as P

EPS = 1e-06
GATE_SCALE = 8.0
MESH = pl.DeviceIdType.MESH
LANES = 256
LINE = 2


def shift_rows(x, d, fill):
    rows = lax.broadcasted_iota(jnp.int32, x.shape, 0)
    return jnp.where(rows < d, fill, pltpu.roll(x, d, 0))


def mixer_body(lin_ref, br_ref, taps_ref, rate_ref, admit_ref, slope_ref, gain_ref, o_ref, a_ref, b_ref):
    length, width = lin_ref.shape
    hd = rate_ref.shape[1]
    linear = lin_ref[...].astype(jnp.float32)
    kernel_len = taps_ref.shape[0]
    filtered = linear * taps_ref[kernel_len - 1 : kernel_len]
    for d in range(1, kernel_len):
        filtered = filtered + shift_rows(linear, d, 0.0) * taps_ref[kernel_len - 1 - d : kernel_len - d]
    narrow = filtered.astype(jnp.bfloat16)
    for j in range(width // hd):
        cols = slice(j * hd, (j + 1) * hd)
        piece = narrow[:, cols]
        rate = jax.nn.sigmoid(jnp.dot(piece, rate_ref[j], preferred_element_type=jnp.float32))
        admit = jax.nn.sigmoid(jnp.dot(piece, admit_ref[j], preferred_element_type=jnp.float32))
        log_decay = rate * slope_ref[:, cols]
        u = 2.0 * log_decay
        decay = jnp.exp(log_decay)
        poly = 1.0 + u * (1.0 / 7.0)
        for c in (6.0, 5.0, 4.0, 3.0, 2.0):
            poly = 1.0 + u * (1.0 / c) * poly
        loss = jnp.where(u > -0.35, -u * poly, 1.0 - decay * decay)
        a = decay
        b = jnp.sqrt(loss) * admit * filtered[:, cols]
        sub = lax.broadcasted_iota(jnp.int32, a.shape, 0) % 8
        for d in (1, 2, 4):
            keep = sub >= d
            pa = jnp.where(keep, pltpu.roll(a, d, 0), 1.0)
            pb = jnp.where(keep, pltpu.roll(b, d, 0), 0.0)
            b = a * pb + b
            a = a * pa
        a_ref[:, cols] = a
        b_ref[:, cols] = b

    def advance(t, carry):
        rows = pl.ds(pl.multiple_of(t * 8, 8), 8)
        s = a_ref[rows, :] * carry + b_ref[rows, :]
        b_ref[rows, :] = s
        return s[7:8, :]

    lax.fori_loop(0, length // 8, advance, jnp.zeros((1, width), jnp.float32), unroll=8)
    for j in range(width // hd):
        cols = slice(j * hd, (j + 1) * hd)
        gated = b_ref[:, cols] * jax.nn.gelu(br_ref[:, cols].astype(jnp.float32))
        scale = lax.rsqrt(jnp.mean(gated * gated, axis=-1, keepdims=True) + EPS)
        o_ref[:, cols] = (gated * scale * gain_ref[:, cols]).astype(o_ref.dtype)


def mixer(linear, branch, taps, rate_blocks, admit_blocks, slope, gain):
    length, channels = linear.shape
    hd = rate_blocks.shape[1]
    per = 2 if rate_blocks.shape[0] % 2 == 0 else 1
    width = per * hd
    wide = pl.BlockSpec((length, width), lambda i: (0, i))
    row = pl.BlockSpec((1, width), lambda i: (0, i))
    blk = pl.BlockSpec((per, hd, hd), lambda i: (i, 0, 0))
    return pl.pallas_call(
        mixer_body,
        grid=(channels // width,),
        in_specs=[wide, wide, pl.BlockSpec((taps.shape[0], width), lambda i: (0, i)), blk, blk, row, row],
        out_specs=wide,
        out_shape=jax.ShapeDtypeStruct((length, channels), jnp.bfloat16),
        scratch_shapes=[pltpu.VMEM((length, width), jnp.float32), pltpu.VMEM((length, width), jnp.float32)],
        cost_estimate=pl.CostEstimate(flops=length * channels * 20000, bytes_accessed=length * channels * 6, transcendentals=0),
        name="mixer",
    )(linear, branch, taps, rate_blocks, admit_blocks, slope, gain)


def ffn_body(g_ref, u_ref, gt_ref, ut_ref, o_ref):
    def conv(ref, taps):
        x = ref[...].astype(jnp.float32)
        n = taps.shape[0]
        y = x * taps[n - 1 : n]
        for d in range(1, n):
            y = y + shift_rows(x, d, 0.0) * taps[n - 1 - d : n - d]
        return y

    o_ref[...] = (jax.nn.silu(conv(g_ref, gt_ref)) * conv(u_ref, ut_ref)).astype(o_ref.dtype)


def ffn_gate(gate_pre, up_pre, gate_taps, up_taps):
    length, units = gate_pre.shape
    width = 128
    wide = pl.BlockSpec((length, width), lambda i: (0, i))
    tap = pl.BlockSpec((gate_taps.shape[0], width), lambda i: (0, i))
    return pl.pallas_call(
        ffn_body,
        grid=(units // width,),
        in_specs=[wide, wide, tap, tap],
        out_specs=wide,
        out_shape=jax.ShapeDtypeStruct((length, units), jnp.bfloat16),
        cost_estimate=pl.CostEstimate(flops=length * units * 8000, bytes_accessed=length * units * 6, transcendentals=0),
        name="ffn_gate",
    )(gate_pre, up_pre, gate_taps, up_taps)


SPLIT = (
    ((8, 8,), (8, 8,),),
    ((8, 8,), (8, 8,),),
    ((8, 8,),),
    ((4, 4,),),
    ((4, 4,),),
    ((8, 5,), (8, 4,), (8, 4,), (8, 4,),),
    ((8, 4,),),
    ((8, 8,),),
)
OPENING = (
    ((0, 1, 0,),),
    ((0, 5, 0,), (0, 6, 0,), (0, 0, 0,),),
    ((1, 6, 1,), (0, 2, 0,), (1, 1, 1,), (0, 3, 0,), (0, 12, 0,), (1, 2, 1,), (1, 1, 2,), (1, 6, 2,), (1, 0, 1,), (1, 2, 2,), (1, 6, 3,), (1, 1, 3,), (0, 11, 0,), (1, 0, 2,), (1, 3, 1,), (1, 5, 2,), (1, 3, 2,),),
    ((2, 0, 0,), (1, 5, 1,), (2, 12, 0,), (1, 5, 3,), (2, 5, 0,), (2, 1, 3,), (0, 4, 0,), (2, 6, 2,), (2, 0, 2,), (2, 2, 1,), (2, 6, 0,), (1, 3, 3,), (2, 6, 3,), (2, 0, 1,), (2, 1, 2,), (2, 1, 1,),),
    ((2, 3, 0,), (1, 2, 3,), (1, 0, 3,), (1, 4, 1,), (1, 4, 2,), (2, 3, 2,), (1, 4, 3,), (1, 12, 1,), (1, 11, 1,), (2, 1, 0,), (2, 4, 0,), (2, 2, 0,), (2, 11, 0,), (2, 5, 1,), (2, 2, 2,), (1, 11, 2,), (2, 2, 3,), (2, 3, 3,), (1, 12, 2,), (2, 5, 2,), (2, 3, 1,), (2, 0, 3,), (0, 10, 0,),),
    ((2, 4, 3,),),
)
MIXING = (
    ((), ((2, 5, 3,), (2, 6, 1,),), ((1, 7, 2,),), ((1, 8, 1,), (1, 7, 3,), (2, 10, 0,), (2, 12, 2,),),),
    (((0, 7, 0,), (0, 9, 0,),), ((2, 4, 2,),), ((1, 8, 2,),), (),),
    ((), ((2, 4, 1,), (0, 8, 0,),), (), (),),
)
SUMMING = (
    (),
    (),
    ((2, 12, 1,), (1, 10, 1,),),
    (),
    (),
    ((2, 11, 1,),),
    (),
    ((1, 7, 1,), (2, 11, 2,),),
    (),
    (),
    (),
    (),
    (),
    (),
    (),
    ((1, 12, 3,), (2, 7, 1,), (1, 10, 2,),),
)
SETTLING = (
    ((1, 9, 1,), (2, 7, 0,), (2, 9, 0,), (2, 8, 0,), (2, 7, 2,), (1, 8, 3,),),
    ((2, 8, 2,), (2, 10, 1,), (1, 11, 3,),),
    ((1, 9, 2,),),
)
ENDING = (
    ((2, 7, 3,),),
    (),
    ((1, 10, 3,), (2, 9, 1,), (2, 12, 3,), (2, 8, 1,),),
    ((1, 9, 3,), (2, 8, 3,), (2, 11, 3,), (2, 10, 2,),),
    ((2, 9, 2,),),
    ((2, 10, 3,),),
    ((2, 9, 3,),),
)


def blocks(heights, widths):
    units = widths[3]
    left = -(-units // (2 * LANES)) * LANES
    span = [(m, heights[m], 0, widths[m]) for m in range(6)]
    span[3:5] = [(m, heights[m], 0, left) for m in (3, 4)]
    return span + [(m, heights[m], left, units - left) for m in (3, 4)]


def plan(spans):
    cuts = []
    for b, (_, rows, _, _) in enumerate(spans):
        parts = len(SPLIT[b])
        step = -(-rows // (128 * parts)) * 128
        cuts.append([(b, at, min(step, rows - at)) + SPLIT[b][i] for i, at in enumerate(range(0, rows, step))])
    pieces = []
    for group in ((0, 1), (2,), (3, 4), (6, 7), (5,)):
        for i in range(max(len(cuts[b]) for b in group)):
            pieces += [cuts[b][i] for b in group if i < len(cuts[b])]
    return pieces


def nearest(depth):
    return [sorted(range(depth), key=lambda s: (abs(s - z), -s)) for z in range(depth)]


def choose(values, at):
    out = jnp.int32(values[0])
    for i, v in enumerate(values[1:], 1):
        out = jnp.where(at == i, jnp.int32(v), out)
    return out


def layer_body(depth, spans, pieces, x_ref, mix_gain, lin_hbm, br_hbm, taps_ref, rate_ref, admit_ref, logit_ref,
               mix_out_gain, out_hbm, ffn_gain, gate_hbm, up_hbm, gtap_ref, utap_ref, down_hbm, o_ref,
               w_lin, w_br, w_out, w_gate, w_up, w_down, peer, normed, mixed, kept, sent, got, middle, hidden,
               a_ref, b_ref, visit, toward, inward, local_sem, z_send, z_extra, z_recv, y_send, y_recv, p_send, p_recv, q_send, q_recv,
               pair_send, pair_recv, sum_send, sum_recv, end_send, end_recv, visit_send, visit_recv, part_send, part_recv):
    x = lax.axis_index("rep")
    f_own = lax.axis_index("fs")
    tp = lax.axis_index("tp")
    z, y = f_own // LINE, f_own % LINE
    length, share = x_ref.shape
    order = nearest(depth)
    hbm = (lin_hbm, br_hbm, out_hbm, gate_hbm, up_hbm, down_hbm)
    full = (w_lin, w_br, w_out, w_gate, w_up, w_down)
    flat = tuple(len(w.shape) == 2 for w in full)
    height = tuple(w.shape[0] // (LINE * depth) if flat[m] else w.shape[1] for m, w in enumerate(full))
    half = w_lin.shape[1]

    def line(s, row):
        return s * LINE + row

    def near(k):
        return choose([order[i][k] for i in range(depth)], z)

    def view(p, f, start, size):
        b, row0 = pieces[p][:2]
        m, _, col, width = spans[b]
        start = pl.multiple_of(row0 + start, 16)
        if flat[m]:
            return full[m].at[pl.ds(pl.multiple_of(f * height[m] + start, 16), size), pl.ds(col, width)]
        return full[m].at[f, pl.ds(start, size), :]

    def parts(p):
        q, (u, v) = pieces[p][2] // 8, pieces[p][3:]
        return {
            "z": ((8 - u) * q * x, u * q),
            "y": ((8 - v) * q * x, v * q),
            "p_out": (u * q * x, (8 - u) * q),
            "p_in": (u * q * (1 - x), (8 - u) * q),
            "q_out": (v * q * x, (8 - v) * q),
            "q_in": (v * q * (1 - x), (8 - v) * q),
        }

    def spare(p, side):
        return pieces[p][3 + side] < 8

    def push(p, f, part, send, recv, device):
        ref = view(p, f, *parts(p)[part])
        return pltpu.make_async_remote_copy(
            src_ref=ref, dst_ref=ref, send_sem=send, recv_sem=recv, device_id=device, device_id_type=MESH
        )

    def own_copy(m):
        src = hbm[m]
        if m < 2:
            src = src.at[:, pl.ds(pl.multiple_of(x * half, LANES), half)]
        if m == 2:
            src = src.at[pl.ds(pl.multiple_of(x * half, LANES), half), :]
        dst = full[m].at[pl.ds(pl.multiple_of(f_own * height[m], 16), height[m]), :] if flat[m] else full[m].at[f_own]
        return pltpu.make_async_copy(src, dst, local_sem.at[m])

    def own(p):
        @pl.when(z < depth - 1)
        def _():
            push(p, f_own, "z", z_send.at[p, z], z_recv.at[p, z], {"fs": line(z + 1, y)}).start()

        @pl.when(z > 0)
        def _():
            push(p, f_own, "z", z_extra.at[p], z_recv.at[p, z], {"fs": line(z - 1, y)}).start()

        push(p, f_own, "y", y_send.at[p, z], y_recv.at[p, z], {"fs": line(z, 1 - y)}).start()

    def along(p, k):
        s = near(k)
        f = line(s, y)
        push(p, f, "z", z_send.at[p, s], z_recv.at[p, s], {"fs": f_own}).wait_recv()
        onward = jnp.where(s < z, z + 1, z - 1)

        @pl.when(jnp.logical_and(onward >= 0, onward < depth))
        def _():
            push(p, f, "z", z_send.at[p, s], z_recv.at[p, s], {"fs": line(onward, y)}).start()

        push(p, f, "y", y_send.at[p, s], y_recv.at[p, s], {"fs": line(z, 1 - y)}).start()
        if spare(p, 0):
            push(p, f, "p_out", p_send.at[p, s], p_recv.at[p, s], {"rep": 1 - x}).start()

    def over(p, k):
        s = near(k)
        f = line(s, 1 - y)
        push(p, f, "y", y_send.at[p, s], y_recv.at[p, s], {"fs": f_own}).wait_recv()
        if spare(p, 1):
            push(p, f, "q_out", q_send.at[p, s], q_recv.at[p, s], {"rep": 1 - x}).start()

    def landed(p, k):
        s = near(k)
        if k and spare(p, 0):
            push(p, line(s, y), "p_in", p_send.at[p, s], p_recv.at[p, s], {"rep": 1 - x}).wait_recv()

    def landed_across(p, k):
        s = near(k)
        if spare(p, 1):
            push(p, line(s, 1 - y), "q_in", q_send.at[p, s], q_recv.at[p, s], {"rep": 1 - x}).wait_recv()

    def complete(m):
        for p, piece in enumerate(pieces):
            if piece[0] == m:
                for k in range(depth):
                    landed(p, k)
                    landed_across(p, k)

    def drain(p):
        @pl.when(z < depth - 1)
        def _():
            push(p, f_own, "z", z_send.at[p, z], z_recv.at[p, z], {"fs": f_own}).wait_send()

        @pl.when(z > 0)
        def _():
            push(p, f_own, "z", z_extra.at[p], z_recv.at[p, z], {"fs": f_own}).wait_send()

        for k in range(depth):
            s = near(k)
            f = line(s, y)
            push(p, f, "y", y_send.at[p, s], y_recv.at[p, s], {"fs": f_own}).wait_send()
            if spare(p, 1):
                push(p, line(s, 1 - y), "q_out", q_send.at[p, s], q_recv.at[p, s], {"fs": f_own}).wait_send()
            if k:
                if spare(p, 0):
                    push(p, f, "p_out", p_send.at[p, s], p_recv.at[p, s], {"fs": f_own}).wait_send()
                onward = jnp.where(s < z, z + 1, z - 1)

                @pl.when(jnp.logical_and(onward >= 0, onward < depth))
                def _():
                    push(p, f, "z", z_send.at[p, s], z_recv.at[p, s], {"fs": f_own}).wait_send()

    count = len(pieces)

    def run(events):
        for kind, p, k in events:
            if kind == 0:
                own(p)
            elif kind == 1:
                along(p, k)
            else:
                over(p, k)

    def slots(step, groups):
        for i, events in enumerate(groups):
            if events:
                pl.when(step == i)(functools.partial(run, events))

    def pair_copy(i, src, dst):
        return pltpu.make_async_remote_copy(
            src_ref=src, dst_ref=dst, send_sem=pair_send.at[i], recv_sem=pair_recv.at[i],
            device_id={"tp": 1 - tp}, device_id_type=MESH,
        )

    def normalize(mine, theirs, gain, target):
        def chunk(i, carry):
            rows = pl.ds(pl.multiple_of(i * 128, 128), 128)
            a = mine[rows, :].astype(jnp.float32)
            b = theirs[rows, :].astype(jnp.float32)
            total = jnp.sum(a * a, axis=-1, keepdims=True) + jnp.sum(b * b, axis=-1, keepdims=True)
            scale = lax.rsqrt(total / (2 * share) + EPS)
            here = pl.ds(pl.multiple_of(tp * share, LANES), share)
            there = pl.ds(pl.multiple_of((1 - tp) * share, LANES), share)
            target[rows, here] = (a * scale * gain[:, here]).astype(jnp.bfloat16)
            target[rows, there] = (b * scale * gain[:, there]).astype(jnp.bfloat16)
            return carry

        lax.fori_loop(0, length // 128, chunk, 0)

    def project(left, right):
        return jnp.dot(left, right, preferred_element_type=jnp.float32).astype(jnp.bfloat16)

    tiles = half // LANES

    def mix(s, j):
        cols = pl.ds(pl.multiple_of(j * LANES, LANES), LANES)
        wide = pl.ds(pl.multiple_of(x * half + j * LANES, LANES), LANES)
        hd = rate_ref.shape[1]
        step = s * tiles + j
        slots(step, MIXING[0])
        linear = project(normed[s], w_lin[:, cols]).astype(jnp.float32)
        kernel_len = taps_ref.shape[0]
        filtered = linear * taps_ref[kernel_len - 1 : kernel_len, wide]
        for d in range(1, kernel_len):
            filtered = filtered + shift_rows(linear, d, 0.0) * taps_ref[kernel_len - 1 - d : kernel_len - d, wide]
        narrow = filtered.astype(jnp.bfloat16)
        for i in range(LANES // hd):
            part = slice(i * hd, (i + 1) * hd)
            lanes = pl.ds(pl.multiple_of(x * half + j * LANES + i * hd, hd), hd)
            block = x * (half // hd) + j * (LANES // hd) + i
            piece = narrow[:, part]
            rate = jax.nn.sigmoid(jnp.dot(piece, rate_ref[block], preferred_element_type=jnp.float32))
            admit = jax.nn.sigmoid(jnp.dot(piece, admit_ref[block], preferred_element_type=jnp.float32))
            logit = logit_ref[:, lanes]
            slope = -GATE_SCALE * (jnp.maximum(-logit, 0.0) + jnp.log1p(jnp.exp(-jnp.abs(logit))))
            log_decay = rate * slope
            u = 2.0 * log_decay
            a = jnp.exp(log_decay)
            poly = 1.0 + u * (1.0 / 7.0)
            for c in (6.0, 5.0, 4.0, 3.0, 2.0):
                poly = 1.0 + u * (1.0 / c) * poly
            loss = jnp.where(u > -0.35, -u * poly, 1.0 - a * a)
            b = jnp.sqrt(loss) * admit * filtered[:, part]
            sub = lax.broadcasted_iota(jnp.int32, a.shape, 0) % 8
            for d in (1, 2, 4):
                keep = sub >= d
                pa = jnp.where(keep, pltpu.roll(a, d, 0), 1.0)
                pb = jnp.where(keep, pltpu.roll(b, d, 0), 0.0)
                b = a * pb + b
                a = a * pa
            a_ref[:, part] = a
            b_ref[:, part] = b
        slots(step, MIXING[1])

        def advance(t, carry):
            rows = pl.ds(pl.multiple_of(t * 8, 8), 8)
            s = a_ref[rows, :] * carry + b_ref[rows, :]
            b_ref[rows, :] = s
            return s[7:8, :]

        lax.fori_loop(0, length // 8, advance, jnp.zeros((1, LANES), jnp.float32), unroll=8)
        slots(step, MIXING[2])
        branch = project(normed[s], w_br[:, cols])
        for i in range(LANES // hd):
            part = slice(i * hd, (i + 1) * hd)
            lanes = pl.ds(pl.multiple_of(x * half + j * LANES + i * hd, hd), hd)
            local = pl.ds(pl.multiple_of(j * LANES + i * hd, hd), hd)
            gated = b_ref[:, part] * jax.nn.gelu(branch[:, part].astype(jnp.float32))
            scale = lax.rsqrt(jnp.mean(gated * gated, axis=-1, keepdims=True) + EPS)
            mixed[:, local] = (gated * scale * mix_out_gain[:, lanes]).astype(mixed.dtype)

    def feed(col, width):
        cols = pl.ds(col, width)

        def conv(weight, taps):
            v = project(normed[0], weight[:, cols]).astype(jnp.float32)
            n = taps.shape[0]
            out = v * taps[n - 1 : n, cols]
            for d in range(1, n):
                out = out + shift_rows(v, d, 0.0) * taps[n - 1 - d : n - d, cols]
            return out

        hidden[:, cols] = (jax.nn.silu(conv(w_gate, gtap_ref)) * conv(w_up, utap_ref)).astype(hidden.dtype)

    per = kept.shape[0]

    def share_out(f, left, weight, s, send, recv):
        result = project(left[...], weight[f])
        slot = f % per

        @pl.when(f // per == tp)
        def _():
            kept[slot] = result

        @pl.when(f // per != tp)
        def _():
            sent[slot] = result
            part_copy(slot, s, send, recv).start()

    def part_copy(slot, s, send, recv):
        return pltpu.make_async_remote_copy(
            src_ref=sent.at[slot], dst_ref=got.at[s, slot], send_sem=send.at[s, slot], recv_sem=recv.at[s, slot],
            device_id={"tp": 1 - tp}, device_id_type=MESH,
        )

    def swap_copy(src, dst, send, recv):
        return pltpu.make_async_remote_copy(
            src_ref=src, dst_ref=dst, send_sem=send, recv_sem=recv, device_id={"rep": 1 - x}, device_id_type=MESH
        )

    def visit_copy():
        return swap_copy(x_ref, visit, visit_send, visit_recv)

    def toward_copy(i):
        return swap_copy(toward.at[i], inward.at[i], part_send.at[i], part_recv.at[i])

    def summed(i, s):
        return kept[i].astype(jnp.float32) + got[s, i].astype(jnp.float32)

    for m in range(6):
        own_copy(m).start()
    barrier = pltpu.get_barrier_semaphore()
    for device in ({"rep": 1 - x}, {"fs": line(z, 1 - y)}, {"tp": 1 - tp}):
        pl.semaphore_signal(barrier, inc=1, device_id=device, device_id_type=MESH)

    @pl.when(z > 0)
    def _():
        pl.semaphore_signal(barrier, inc=1, device_id={"fs": line(z - 1, y)}, device_id_type=MESH)

    @pl.when(z < depth - 1)
    def _():
        pl.semaphore_signal(barrier, inc=1, device_id={"fs": line(z + 1, y)}, device_id_type=MESH)

    pl.semaphore_wait(barrier, 3 + jnp.where(z > 0, 1, 0) + jnp.where(z < depth - 1, 1, 0))

    ready = []

    def prepare(events):
        for event in events:
            m = spans[pieces[event[1]][0]][0]
            if event[0] == 0 and m not in ready:
                own_copy(m).wait()
                ready.append(m)
            run((event,))

    prepare(OPENING[0])
    visit_copy().start()
    pair_copy(0, x_ref, peer.at[0]).start()
    prepare(OPENING[1])
    pair_copy(0, x_ref, peer.at[0]).wait()
    normalize(x_ref, peer.at[0], mix_gain, normed.at[1])
    prepare(OPENING[2])
    visit_copy().wait()
    pair_copy(1, visit, peer.at[1]).start()
    prepare(OPENING[3])
    pair_copy(1, visit, peer.at[1]).wait()
    normalize(visit, peer.at[1], mix_gain, normed.at[0])
    prepare(OPENING[4])
    for m in range(6):
        if m not in ready:
            own_copy(m).wait()
    complete(0)
    complete(1)

    @pl.loop(0, 2)
    def _(s):
        pl.loop(0, tiles)(lambda j: mix(s, j))

        @pl.when(s == 0)
        def _():
            run(OPENING[5])
            complete(2)

        @pl.loop(0, 2 * per)
        def _(f):
            slots(s * 2 * per + f, SUMMING)
            share_out(f, mixed, w_out, s, sum_send, sum_recv)

        for i in range(per):
            part_copy(i, s, sum_send, sum_recv).wait_send()
            part_copy(i, s, sum_send, sum_recv).wait_recv()

            @pl.when(s == 0)
            def _():
                toward[i] = summed(i, 0).astype(jnp.bfloat16)
                toward_copy(i).start()

    run(SETTLING[0])
    for i in range(per):
        cols = slice(i * LANES, (i + 1) * LANES)
        toward_copy(i).wait_recv()
        total = summed(i, 1) + inward[i].astype(jnp.float32)
        middle[:, cols] = (x_ref[:, cols].astype(jnp.float32) + total).astype(middle.dtype)
    pair_copy(2, middle, peer.at[0]).start()
    run(SETTLING[1])
    pair_copy(2, middle, peer.at[0]).wait()
    normalize(middle, peer.at[0], ffn_gain, normed.at[0])
    run(SETTLING[2])
    complete(3)
    complete(4)
    units = hidden.shape[1]
    wide = units // LANES

    @pl.loop(0, wide)
    def _(j):
        slots(j, ENDING[:wide])

        @pl.when(j == spans[6][2] // LANES)
        def _():
            complete(6)
            complete(7)

        feed(pl.multiple_of(j * LANES, LANES), LANES)

    for events in ENDING[wide:-1]:
        run(events)
    if units % LANES:
        feed(wide * LANES, units % LANES)
    run(ENDING[-1])

    @pl.loop(0, 2 * depth)
    def _(t):
        for k in range(depth):
            for side, waits in enumerate((landed, landed_across)):
                @pl.when(t == 2 * k + side)
                def _():
                    for p, piece in enumerate(pieces):
                        if piece[0] == 5:
                            waits(p, k)
        s = choose([order[i][0] for i in range(depth)], z)
        for k in range(1, depth):
            s = jnp.where(t // 2 == k, near(k), s)
        f = jnp.where(t % 2 == 0, line(s, y), line(s, 1 - y))
        share_out(f, hidden, w_down, 0, end_send, end_recv)

    for i in range(per):
        cols = slice(i * LANES, (i + 1) * LANES)
        part_copy(i, 0, end_send, end_recv).wait_recv()
        o_ref[:, cols] = (middle[:, cols].astype(jnp.float32) + summed(i, 0)).astype(o_ref.dtype)
    for i in range(per):
        part_copy(i, 0, end_send, end_recv).wait_send()
        toward_copy(i).wait_send()
    for p in range(count):
        drain(p)


def fused(depth, stream_in, mix_gain, lin_weight, branch_weight, lin_taps, rate_blocks, admit_blocks, decay_logit,
          mix_out_gain, out_weight, ffn_gain, gate_weight, up_weight, gate_taps, up_taps, down_weight):
    own = stream_in[0]
    length, share = own.shape
    n = LINE * depth
    shards = (lin_weight, branch_weight, out_weight, gate_weight, up_weight, down_weight)
    half = lin_weight.shape[1] // 2
    heights = [half if m == 2 else w.shape[0] for m, w in enumerate(shards)]
    widths = [half if m < 2 else w.shape[1] for m, w in enumerate(shards)]
    spans = blocks(heights, widths)
    pieces = plan(spans)
    bf = jnp.bfloat16
    whole = [
        pltpu.VMEM((n, h, w), bf) if m in (2, 5) else pltpu.VMEM((n * h, w), bf)
        for m, (h, w) in enumerate(zip(heights, widths))
    ]
    units = gate_weight.shape[1]
    width = out_weight.shape[1]
    count = len(pieces)
    dma = pltpu.SemaphoreType.DMA
    scratch = whole + [
        pltpu.VMEM((2, length, share), bf),
        pltpu.VMEM((2, length, 2 * share), bf),
        pltpu.VMEM((length, half), bf),
        pltpu.VMEM((n // 2, length, width), bf),
        pltpu.VMEM((n // 2, length, width), bf),
        pltpu.VMEM((2, n // 2, length, width), bf),
        pltpu.VMEM((length, share), bf),
        pltpu.VMEM((length, units), bf),
        pltpu.VMEM((length, LANES), jnp.float32),
        pltpu.VMEM((length, LANES), jnp.float32),
        pltpu.VMEM((length, share), bf),
        pltpu.VMEM((n // 2, length, width), bf),
        pltpu.VMEM((n // 2, length, width), bf),
        dma((6,)),
        dma((count, depth)),
        dma((count,)),
        dma((count, depth)),
        dma((count, depth)),
        dma((count, depth)),
        dma((count, depth)),
        dma((count, depth)),
        dma((count, depth)),
        dma((count, depth)),
        dma((3,)),
        dma((3,)),
        dma((2, n // 2)),
        dma((2, n // 2)),
        dma((1, n // 2)),
        dma((1, n // 2)),
        dma,
        dma,
        dma((n // 2,)),
        dma((n // 2,)),
    ]
    near = pl.BlockSpec(memory_space=pltpu.VMEM)
    far = pl.BlockSpec(memory_space=pl.ANY)
    macs = length * share * 2 * (3 * share + 3 * units)
    result = pl.pallas_call(
        functools.partial(layer_body, depth, spans, pieces),
        in_specs=[near, near, far, far, near, near, near, near, near, far, near, far, far, near, near, far],
        out_specs=near,
        out_shape=jax.ShapeDtypeStruct((length, share), bf),
        scratch_shapes=scratch,
        compiler_params=pltpu.CompilerParams(collective_id=0, has_side_effects=True, vmem_limit_bytes=67043328),
        cost_estimate=pl.CostEstimate(flops=2 * macs, bytes_accessed=2 * macs // length, transcendentals=0),
        name="layer",
    )(own, mix_gain.reshape(1, -1), lin_weight, branch_weight, lin_taps, rate_blocks, admit_blocks, decay_logit.reshape(1, -1),
      mix_out_gain.reshape(1, -1), out_weight, ffn_gain.reshape(1, -1), gate_weight, up_weight, gate_taps,
      up_taps, down_weight)
    return result[None]


def gathered(tps, stream_in, mix_gain, lin_weight, branch_weight, lin_taps, rate_blocks, admit_blocks,
             decay_logit, mix_out_gain, out_weight, ffn_gain, gate_weight, up_weight, gate_taps, up_taps, down_weight):
    own = stream_in[0]
    length, share = own.shape

    def normed_rows(mine, gain):
        pair = lax.all_gather(mine, "tp", axis=0).astype(jnp.float32)
        mean_sq = jnp.sum(pair * pair, axis=(0, 2), keepdims=True) / (tps * share)
        y = (pair * lax.rsqrt(mean_sq + EPS) * gain.reshape(tps, 1, share)).astype(jnp.bfloat16)
        return y.transpose(1, 0, 2).reshape(length, tps * share)

    def product(left, right):
        return jnp.dot(left, right, preferred_element_type=jnp.float32).astype(jnp.bfloat16)

    def scatter(left, right):
        stack = product(left, right).reshape(length, tps, share).transpose(1, 0, 2)
        if tps == 2:
            tp = lax.axis_index("tp")
            mine = lax.dynamic_index_in_dim(stack, tp, 0, keepdims=False)
            other = lax.dynamic_index_in_dim(stack, 1 - tp, 0, keepdims=False)
            other = lax.ppermute(other, "tp", [(0, 1), (1, 0)])
            return mine.astype(jnp.float32) + other.astype(jnp.float32)
        return lax.psum_scatter(stack, "tp", scatter_dimension=0, tiled=False).astype(jnp.float32)

    def gather(w, axis=0):
        return lax.all_gather(w, "fs", axis=axis, tiled=True)

    normed = normed_rows(own, mix_gain)
    linear = product(normed, gather(lin_weight))
    branch = product(normed, gather(branch_weight))
    slope = (-GATE_SCALE * jax.nn.softplus(-decay_logit)).reshape(1, -1)
    mixed = mixer(linear, branch, lin_taps, rate_blocks, admit_blocks, slope, mix_out_gain.reshape(1, -1))
    middle = (own.astype(jnp.float32) + scatter(mixed, gather(out_weight, 1))).astype(jnp.bfloat16)
    normed2 = normed_rows(middle, ffn_gain)
    gate_pre = product(normed2, gather(gate_weight))
    up_pre = product(normed2, gather(up_weight))
    hidden = ffn_gate(gate_pre, up_pre, gate_taps, up_taps)
    result = (middle.astype(jnp.float32) + scatter(hidden, gather(down_weight, 1))).astype(jnp.bfloat16)
    return result[None]


def solution(mesh):
    placed = (
        P(("rep", "fs"), None, "tp"),
        P(),
        P("fs", "tp"),
        P("fs", "tp"),
        P(None, "tp"),
        P("tp", None, None),
        P("tp", None, None),
        P("tp"),
        P("tp"),
        P("tp", "fs"),
        P(),
        P("fs", "tp"),
        P("fs", "tp"),
        P(None, "tp"),
        P(None, "tp"),
        P("tp", "fs"),
    )
    reps, n, tps = mesh.shape["rep"], mesh.shape["fs"], mesh.shape["tp"]
    if reps == 2 and tps == 2 and n == 8:
        body = functools.partial(fused, n // LINE)
    else:
        body = functools.partial(gathered, tps)
    return jax.shard_map(
        body, mesh=mesh, in_specs=placed, out_specs=P(("rep", "fs"), None, "tp"), check_vma=False
    )
```

```python
import functools

import jax
import jax.numpy as jnp
from jax import lax
from jax.experimental import pallas as pl
from jax.experimental.pallas import tpu as pltpu
from jax.sharding import PartitionSpec as P

EPS = 1e-06
GATE_SCALE = 8.0
MESH = pl.DeviceIdType.MESH
LANES = 256
LINE = 2


def shift_rows(x, d, fill):
    rows = lax.broadcasted_iota(jnp.int32, x.shape, 0)
    return jnp.where(rows < d, fill, pltpu.roll(x, d, 0))


def mixer_body(lin_ref, br_ref, taps_ref, rate_ref, admit_ref, slope_ref, gain_ref, o_ref, a_ref, b_ref):
    length, width = lin_ref.shape
    hd = rate_ref.shape[1]
    linear = lin_ref[...].astype(jnp.float32)
    kernel_len = taps_ref.shape[0]
    filtered = linear * taps_ref[kernel_len - 1 : kernel_len]
    for d in range(1, kernel_len):
        filtered = filtered + shift_rows(linear, d, 0.0) * taps_ref[kernel_len - 1 - d : kernel_len - d]
    narrow = filtered.astype(jnp.bfloat16)
    for j in range(width // hd):
        cols = slice(j * hd, (j + 1) * hd)
        piece = narrow[:, cols]
        rate = jax.nn.sigmoid(jnp.dot(piece, rate_ref[j], preferred_element_type=jnp.float32))
        admit = jax.nn.sigmoid(jnp.dot(piece, admit_ref[j], preferred_element_type=jnp.float32))
        log_decay = rate * slope_ref[:, cols]
        u = 2.0 * log_decay
        decay = jnp.exp(log_decay)
        poly = 1.0 + u * (1.0 / 7.0)
        for c in (6.0, 5.0, 4.0, 3.0, 2.0):
            poly = 1.0 + u * (1.0 / c) * poly
        loss = jnp.where(u > -0.35, -u * poly, 1.0 - decay * decay)
        a = decay
        b = jnp.sqrt(loss) * admit * filtered[:, cols]
        sub = lax.broadcasted_iota(jnp.int32, a.shape, 0) % 8
        for d in (1, 2, 4):
            keep = sub >= d
            pa = jnp.where(keep, pltpu.roll(a, d, 0), 1.0)
            pb = jnp.where(keep, pltpu.roll(b, d, 0), 0.0)
            b = a * pb + b
            a = a * pa
        a_ref[:, cols] = a
        b_ref[:, cols] = b

    def advance(t, carry):
        rows = pl.ds(pl.multiple_of(t * 8, 8), 8)
        s = a_ref[rows, :] * carry + b_ref[rows, :]
        b_ref[rows, :] = s
        return s[7:8, :]

    lax.fori_loop(0, length // 8, advance, jnp.zeros((1, width), jnp.float32), unroll=8)
    for j in range(width // hd):
        cols = slice(j * hd, (j + 1) * hd)
        gated = b_ref[:, cols] * jax.nn.gelu(br_ref[:, cols].astype(jnp.float32))
        scale = lax.rsqrt(jnp.mean(gated * gated, axis=-1, keepdims=True) + EPS)
        o_ref[:, cols] = (gated * scale * gain_ref[:, cols]).astype(o_ref.dtype)


def mixer(linear, branch, taps, rate_blocks, admit_blocks, slope, gain):
    length, channels = linear.shape
    hd = rate_blocks.shape[1]
    per = 2 if rate_blocks.shape[0] % 2 == 0 else 1
    width = per * hd
    wide = pl.BlockSpec((length, width), lambda i: (0, i))
    row = pl.BlockSpec((1, width), lambda i: (0, i))
    blk = pl.BlockSpec((per, hd, hd), lambda i: (i, 0, 0))
    return pl.pallas_call(
        mixer_body,
        grid=(channels // width,),
        in_specs=[wide, wide, pl.BlockSpec((taps.shape[0], width), lambda i: (0, i)), blk, blk, row, row],
        out_specs=wide,
        out_shape=jax.ShapeDtypeStruct((length, channels), jnp.bfloat16),
        scratch_shapes=[pltpu.VMEM((length, width), jnp.float32), pltpu.VMEM((length, width), jnp.float32)],
        cost_estimate=pl.CostEstimate(flops=length * channels * 20000, bytes_accessed=length * channels * 6, transcendentals=0),
        name="mixer",
    )(linear, branch, taps, rate_blocks, admit_blocks, slope, gain)


def ffn_body(g_ref, u_ref, gt_ref, ut_ref, o_ref):
    def conv(ref, taps):
        x = ref[...].astype(jnp.float32)
        n = taps.shape[0]
        y = x * taps[n - 1 : n]
        for d in range(1, n):
            y = y + shift_rows(x, d, 0.0) * taps[n - 1 - d : n - d]
        return y

    o_ref[...] = (jax.nn.silu(conv(g_ref, gt_ref)) * conv(u_ref, ut_ref)).astype(o_ref.dtype)


def ffn_gate(gate_pre, up_pre, gate_taps, up_taps):
    length, units = gate_pre.shape
    width = 128
    wide = pl.BlockSpec((length, width), lambda i: (0, i))
    tap = pl.BlockSpec((gate_taps.shape[0], width), lambda i: (0, i))
    return pl.pallas_call(
        ffn_body,
        grid=(units // width,),
        in_specs=[wide, wide, tap, tap],
        out_specs=wide,
        out_shape=jax.ShapeDtypeStruct((length, units), jnp.bfloat16),
        cost_estimate=pl.CostEstimate(flops=length * units * 8000, bytes_accessed=length * units * 6, transcendentals=0),
        name="ffn_gate",
    )(gate_pre, up_pre, gate_taps, up_taps)


SPLIT = (
    ((8, 8,), (8, 8,),),
    ((8, 8,), (8, 8,),),
    ((8, 8,),),
    ((4, 4,),),
    ((4, 4,),),
    ((8, 5,), (8, 4,), (8, 4,), (8, 4,),),
    ((8, 4,),),
    ((8, 8,),),
)
OPENING = (
    ((0, 1, 0,),),
    ((0, 5, 0,), (0, 6, 0,), (0, 0, 0,),),
    ((1, 6, 1,), (0, 2, 0,), (1, 1, 1,), (0, 3, 0,), (0, 12, 0,), (1, 2, 1,), (1, 1, 2,), (1, 6, 2,), (1, 0, 1,), (1, 2, 2,), (1, 6, 3,), (1, 1, 3,), (0, 11, 0,), (1, 0, 2,), (1, 3, 1,), (1, 5, 2,), (1, 3, 2,),),
    ((2, 0, 0,), (1, 5, 1,), (2, 12, 0,), (1, 5, 3,), (2, 5, 0,), (2, 1, 3,), (0, 4, 0,), (2, 6, 2,), (2, 0, 2,), (2, 2, 1,), (2, 6, 0,), (1, 3, 3,), (2, 6, 3,), (2, 0, 1,), (2, 1, 2,), (2, 1, 1,),),
    ((2, 3, 0,), (1, 2, 3,), (1, 0, 3,), (1, 4, 1,), (1, 4, 2,), (2, 3, 2,), (1, 4, 3,), (1, 12, 1,), (1, 11, 1,), (2, 1, 0,), (2, 4, 0,), (2, 2, 0,), (2, 11, 0,), (2, 5, 1,), (2, 2, 2,), (1, 11, 2,), (2, 2, 3,), (2, 3, 3,), (1, 12, 2,), (2, 5, 2,), (2, 3, 1,), (2, 0, 3,), (0, 10, 0,),),
    ((2, 4, 3,),),
)
MIXING = (
    ((), ((2, 5, 3,), (2, 6, 1,),), ((1, 7, 2,),), ((1, 8, 1,), (1, 7, 3,), (2, 10, 0,), (2, 12, 2,),),),
    (((0, 7, 0,), (0, 9, 0,),), ((2, 4, 2,),), ((1, 8, 2,),), (),),
    ((), ((2, 4, 1,), (0, 8, 0,),), (), (),),
)
SUMMING = (
    (),
    (),
    ((2, 12, 1,), (1, 10, 1,),),
    (),
    (),
    ((2, 11, 1,),),
    (),
    ((1, 7, 1,), (2, 11, 2,),),
    (),
    (),
    (),
    (),
    (),
    (),
    (),
    ((1, 12, 3,), (2, 7, 1,), (1, 10, 2,),),
)
SETTLING = (
    ((1, 9, 1,), (2, 7, 0,), (2, 9, 0,), (2, 8, 0,), (2, 7, 2,), (1, 8, 3,),),
    ((2, 8, 2,), (2, 10, 1,), (1, 11, 3,),),
    ((1, 9, 2,),),
)
ENDING = (
    ((2, 7, 3,),),
    (),
    ((1, 10, 3,), (2, 9, 1,), (2, 12, 3,), (2, 8, 1,),),
    ((1, 9, 3,), (2, 8, 3,), (2, 11, 3,), (2, 10, 2,),),
    ((2, 9, 2,),),
    ((2, 10, 3,),),
    ((2, 9, 3,),),
)


def blocks(heights, widths):
    units = widths[3]
    left = -(-units // (2 * LANES)) * LANES
    span = [(m, heights[m], 0, widths[m]) for m in range(6)]
    span[3:5] = [(m, heights[m], 0, left) for m in (3, 4)]
    return span + [(m, heights[m], left, units - left) for m in (3, 4)]


def plan(spans):
    cuts = []
    for b, (_, rows, _, _) in enumerate(spans):
        parts = len(SPLIT[b])
        step = -(-rows // (128 * parts)) * 128
        cuts.append([(b, at, min(step, rows - at)) + SPLIT[b][i] for i, at in enumerate(range(0, rows, step))])
    pieces = []
    for group in ((0, 1), (2,), (3, 4), (6, 7), (5,)):
        for i in range(max(len(cuts[b]) for b in group)):
            pieces += [cuts[b][i] for b in group if i < len(cuts[b])]
    return pieces


def nearest(depth):
    return [sorted(range(depth), key=lambda s: (abs(s - z), -s)) for z in range(depth)]


def choose(values, at):
    out = jnp.int32(values[0])
    for i, v in enumerate(values[1:], 1):
        out = jnp.where(at == i, jnp.int32(v), out)
    return out


def layer_body(depth, spans, pieces, x_ref, mix_gain, lin_hbm, br_hbm, taps_ref, rate_ref, admit_ref, logit_ref,
               mix_out_gain, out_hbm, ffn_gain, gate_hbm, up_hbm, gtap_ref, utap_ref, down_hbm, o_ref,
               w_lin, w_br, w_out, w_gate, w_up, w_down, peer, normed, mixed, kept, sent, got, middle, hidden,
               a_ref, b_ref, visit, toward, inward, local_sem, z_send, z_recv, y_send, y_recv, p_send, p_recv, q_send, q_recv,
               pair_send, pair_recv, sum_send, sum_recv, end_send, end_recv, visit_send, visit_recv, part_send, part_recv):
    x = lax.axis_index("rep")
    f_own = lax.axis_index("fs")
    tp = lax.axis_index("tp")
    z, y = f_own // LINE, f_own % LINE
    length, share = x_ref.shape
    order = nearest(depth)
    hbm = (lin_hbm, br_hbm, out_hbm, gate_hbm, up_hbm, down_hbm)
    full = (w_lin, w_br, w_out, w_gate, w_up, w_down)
    flat = tuple(len(w.shape) == 2 for w in full)
    height = tuple(w.shape[0] // (LINE * depth) if flat[m] else w.shape[1] for m, w in enumerate(full))
    half = w_lin.shape[1]

    def line(s, row):
        return s * LINE + row

    def near(k):
        return choose([order[i][k] for i in range(depth)], z)

    def view(p, f, start, size):
        b, row0 = pieces[p][:2]
        m, _, col, width = spans[b]
        start = pl.multiple_of(row0 + start, 16)
        if flat[m]:
            return full[m].at[pl.ds(pl.multiple_of(f * height[m] + start, 16), size), pl.ds(col, width)]
        return full[m].at[f, pl.ds(start, size), :]

    def parts(p):
        q, (u, v) = pieces[p][2] // 8, pieces[p][3:]
        return {
            "z": ((8 - u) * q * x, u * q),
            "y": ((8 - v) * q * x, v * q),
            "p_out": (u * q * x, (8 - u) * q),
            "p_in": (u * q * (1 - x), (8 - u) * q),
            "q_out": (v * q * x, (8 - v) * q),
            "q_in": (v * q * (1 - x), (8 - v) * q),
        }

    def spare(p, side):
        return pieces[p][3 + side] < 8

    def push(p, f, part, send, recv, device):
        ref = view(p, f, *parts(p)[part])
        return pltpu.make_async_remote_copy(
            src_ref=ref, dst_ref=ref, send_sem=send, recv_sem=recv, device_id=device, device_id_type=MESH
        )

    def own_copy(m):
        src = hbm[m]
        if m < 2:
            src = src.at[:, pl.ds(pl.multiple_of(x * half, LANES), half)]
        if m == 2:
            src = src.at[pl.ds(pl.multiple_of(x * half, LANES), half), :]
        dst = full[m].at[pl.ds(pl.multiple_of(f_own * height[m], 16), height[m]), :] if flat[m] else full[m].at[f_own]
        return pltpu.make_async_copy(src, dst, local_sem.at[m])

    def own(p):
        @pl.when(z < depth - 1)
        def _():
            push(p, f_own, "z", z_send.at[p], z_recv.at[p, z], {"fs": line(z + 1, y)}).start()

        @pl.when(z > 0)
        def _():
            push(p, f_own, "z", z_send.at[p], z_recv.at[p, z], {"fs": line(z - 1, y)}).start()

        push(p, f_own, "y", y_send.at[p], y_recv.at[p, z], {"fs": line(z, 1 - y)}).start()

    def along(p, k):
        s = near(k)
        f = line(s, y)
        push(p, f, "z", z_send.at[p], z_recv.at[p, s], {"fs": f_own}).wait_recv()
        onward = jnp.where(s < z, z + 1, z - 1)

        @pl.when(jnp.logical_and(onward >= 0, onward < depth))
        def _():
            push(p, f, "z", z_send.at[p], z_recv.at[p, s], {"fs": line(onward, y)}).start()

        push(p, f, "y", y_send.at[p], y_recv.at[p, s], {"fs": line(z, 1 - y)}).start()
        if spare(p, 0):
            push(p, f, "p_out", p_send.at[p], p_recv.at[p, s], {"rep": 1 - x}).start()

    def over(p, k):
        s = near(k)
        f = line(s, 1 - y)
        push(p, f, "y", y_send.at[p], y_recv.at[p, s], {"fs": f_own}).wait_recv()
        if spare(p, 1):
            push(p, f, "q_out", q_send.at[p], q_recv.at[p, s], {"rep": 1 - x}).start()

    def landed(p, k):
        s = near(k)
        if k and spare(p, 0):
            push(p, line(s, y), "p_in", p_send.at[p], p_recv.at[p, s], {"rep": 1 - x}).wait_recv()

    def landed_across(p, k):
        s = near(k)
        if spare(p, 1):
            push(p, line(s, 1 - y), "q_in", q_send.at[p], q_recv.at[p, s], {"rep": 1 - x}).wait_recv()

    def complete(m):
        for p, piece in enumerate(pieces):
            if piece[0] == m:
                for k in range(depth):
                    landed(p, k)
                    landed_across(p, k)

    def all_sent(p, part, copies, sem):
        b = pieces[p][0]
        m, _, _, width = spans[b]
        rows = parts(p)[part][1]
        if flat[m]:
            ref = full[m].at[pl.ds(0, copies * rows), pl.ds(0, width)]
        else:
            ref = full[m].at[pl.ds(0, copies), pl.ds(0, rows), :]
        pltpu.make_async_remote_copy(
            src_ref=ref, dst_ref=ref, send_sem=sem, recv_sem=sem, device_id={"rep": 1 - x}, device_id_type=MESH
        ).wait_send()

    def drain(p):
        inner = jnp.logical_and(z > 0, z < depth - 1)
        pl.when(inner)(lambda: all_sent(p, "z", depth + 1, z_send.at[p]))
        pl.when(jnp.logical_not(inner))(lambda: all_sent(p, "z", 1, z_send.at[p]))
        all_sent(p, "y", depth, y_send.at[p])
        if spare(p, 0):
            all_sent(p, "p_out", depth - 1, p_send.at[p])
        if spare(p, 1):
            all_sent(p, "q_out", depth, q_send.at[p])

    def drain_all(blocks_done):
        for p, piece in enumerate(pieces):
            if piece[0] in blocks_done:
                drain(p)

    def run(events):
        for kind, p, k in events:
            if kind == 0:
                own(p)
            elif kind == 1:
                along(p, k)
            else:
                over(p, k)

    def slots(step, groups):
        for i, events in enumerate(groups):
            if events:
                pl.when(step == i)(functools.partial(run, events))

    def pair_copy(i, src, dst):
        return pltpu.make_async_remote_copy(
            src_ref=src, dst_ref=dst, send_sem=pair_send.at[i], recv_sem=pair_recv.at[i],
            device_id={"tp": 1 - tp}, device_id_type=MESH,
        )

    def normalize(mine, theirs, gain, target):
        def chunk(i, carry):
            rows = pl.ds(pl.multiple_of(i * 128, 128), 128)
            a = mine[rows, :].astype(jnp.float32)
            b = theirs[rows, :].astype(jnp.float32)
            total = jnp.sum(a * a, axis=-1, keepdims=True) + jnp.sum(b * b, axis=-1, keepdims=True)
            scale = lax.rsqrt(total / (2 * share) + EPS)
            here = pl.ds(pl.multiple_of(tp * share, LANES), share)
            there = pl.ds(pl.multiple_of((1 - tp) * share, LANES), share)
            target[rows, here] = (a * scale * gain[:, here]).astype(jnp.bfloat16)
            target[rows, there] = (b * scale * gain[:, there]).astype(jnp.bfloat16)
            return carry

        lax.fori_loop(0, length // 128, chunk, 0)

    def project(left, right):
        return jnp.dot(left, right, preferred_element_type=jnp.float32).astype(jnp.bfloat16)

    tiles = half // LANES

    def mix(s, j):
        cols = pl.ds(pl.multiple_of(j * LANES, LANES), LANES)
        wide = pl.ds(pl.multiple_of(x * half + j * LANES, LANES), LANES)
        hd = rate_ref.shape[1]
        step = s * tiles + j
        slots(step, MIXING[0])
        linear = project(normed[s], w_lin[:, cols]).astype(jnp.float32)
        kernel_len = taps_ref.shape[0]
        filtered = linear * taps_ref[kernel_len - 1 : kernel_len, wide]
        for d in range(1, kernel_len):
            filtered = filtered + shift_rows(linear, d, 0.0) * taps_ref[kernel_len - 1 - d : kernel_len - d, wide]
        narrow = filtered.astype(jnp.bfloat16)
        for i in range(LANES // hd):
            part = slice(i * hd, (i + 1) * hd)
            lanes = pl.ds(pl.multiple_of(x * half + j * LANES + i * hd, hd), hd)
            block = x * (half // hd) + j * (LANES // hd) + i
            piece = narrow[:, part]
            rate = jax.nn.sigmoid(jnp.dot(piece, rate_ref[block], preferred_element_type=jnp.float32))
            admit = jax.nn.sigmoid(jnp.dot(piece, admit_ref[block], preferred_element_type=jnp.float32))
            logit = logit_ref[:, lanes]
            slope = -GATE_SCALE * (jnp.maximum(-logit, 0.0) + jnp.log1p(jnp.exp(-jnp.abs(logit))))
            log_decay = rate * slope
            u = 2.0 * log_decay
            a = jnp.exp(log_decay)
            poly = 1.0 + u * (1.0 / 7.0)
            for c in (6.0, 5.0, 4.0, 3.0, 2.0):
                poly = 1.0 + u * (1.0 / c) * poly
            loss = jnp.where(u > -0.35, -u * poly, 1.0 - a * a)
            b = jnp.sqrt(loss) * admit * filtered[:, part]
            sub = lax.broadcasted_iota(jnp.int32, a.shape, 0) % 8
            for d in (1, 2, 4):
                keep = sub >= d
                pa = jnp.where(keep, pltpu.roll(a, d, 0), 1.0)
                pb = jnp.where(keep, pltpu.roll(b, d, 0), 0.0)
                b = a * pb + b
                a = a * pa
            a_ref[:, part] = a
            b_ref[:, part] = b
        slots(step, MIXING[1])

        def advance(t, carry):
            rows = pl.ds(pl.multiple_of(t * 8, 8), 8)
            s = a_ref[rows, :] * carry + b_ref[rows, :]
            b_ref[rows, :] = s
            return s[7:8, :]

        lax.fori_loop(0, length // 8, advance, jnp.zeros((1, LANES), jnp.float32), unroll=8)
        slots(step, MIXING[2])
        branch = project(normed[s], w_br[:, cols])
        for i in range(LANES // hd):
            part = slice(i * hd, (i + 1) * hd)
            lanes = pl.ds(pl.multiple_of(x * half + j * LANES + i * hd, hd), hd)
            local = pl.ds(pl.multiple_of(j * LANES + i * hd, hd), hd)
            gated = b_ref[:, part] * jax.nn.gelu(branch[:, part].astype(jnp.float32))
            scale = lax.rsqrt(jnp.mean(gated * gated, axis=-1, keepdims=True) + EPS)
            mixed[:, local] = (gated * scale * mix_out_gain[:, lanes]).astype(mixed.dtype)

    def feed(col, width):
        cols = pl.ds(col, width)

        def conv(weight, taps):
            v = project(normed[0], weight[:, cols]).astype(jnp.float32)
            n = taps.shape[0]
            out = v * taps[n - 1 : n, cols]
            for d in range(1, n):
                out = out + shift_rows(v, d, 0.0) * taps[n - 1 - d : n - d, cols]
            return out

        hidden[:, cols] = (jax.nn.silu(conv(w_gate, gtap_ref)) * conv(w_up, utap_ref)).astype(hidden.dtype)

    per = kept.shape[0]

    def share_out(f, left, weight, s, send, recv):
        result = project(left[...], weight[f])
        slot = f % per

        @pl.when(f // per == tp)
        def _():
            kept[slot] = result

        @pl.when(f // per != tp)
        def _():
            sent[slot] = result
            part_copy(slot, s, send, recv).start()

    def part_copy(slot, s, send, recv):
        return pltpu.make_async_remote_copy(
            src_ref=sent.at[slot], dst_ref=got.at[s, slot], send_sem=send.at[s, slot], recv_sem=recv.at[s, slot],
            device_id={"tp": 1 - tp}, device_id_type=MESH,
        )

    def swap_copy(src, dst, send, recv):
        return pltpu.make_async_remote_copy(
            src_ref=src, dst_ref=dst, send_sem=send, recv_sem=recv, device_id={"rep": 1 - x}, device_id_type=MESH
        )

    def visit_copy():
        return swap_copy(x_ref, visit, visit_send, visit_recv)

    def toward_copy(i):
        return swap_copy(toward.at[i], inward.at[i], part_send.at[i], part_recv.at[i])

    def summed(i, s):
        return kept[i].astype(jnp.float32) + got[s, i].astype(jnp.float32)

    for m in range(6):
        own_copy(m).start()
    barrier = pltpu.get_barrier_semaphore()
    for device in ({"rep": 1 - x}, {"fs": line(z, 1 - y)}, {"tp": 1 - tp}):
        pl.semaphore_signal(barrier, inc=1, device_id=device, device_id_type=MESH)

    @pl.when(z > 0)
    def _():
        pl.semaphore_signal(barrier, inc=1, device_id={"fs": line(z - 1, y)}, device_id_type=MESH)

    @pl.when(z < depth - 1)
    def _():
        pl.semaphore_signal(barrier, inc=1, device_id={"fs": line(z + 1, y)}, device_id_type=MESH)

    pl.semaphore_wait(barrier, 3 + jnp.where(z > 0, 1, 0) + jnp.where(z < depth - 1, 1, 0))

    ready = []

    def prepare(events):
        for event in events:
            m = spans[pieces[event[1]][0]][0]
            if event[0] == 0 and m not in ready:
                own_copy(m).wait()
                ready.append(m)
            run((event,))

    prepare(OPENING[0])
    visit_copy().start()
    pair_copy(0, x_ref, peer.at[0]).start()
    prepare(OPENING[1])
    pair_copy(0, x_ref, peer.at[0]).wait()
    normalize(x_ref, peer.at[0], mix_gain, normed.at[1])
    prepare(OPENING[2])
    visit_copy().wait()
    pair_copy(1, visit, peer.at[1]).start()
    prepare(OPENING[3])
    pair_copy(1, visit, peer.at[1]).wait()
    normalize(visit, peer.at[1], mix_gain, normed.at[0])
    prepare(OPENING[4])
    for m in range(6):
        if m not in ready:
            own_copy(m).wait()
    complete(0)
    complete(1)

    @pl.loop(0, 2)
    def _(s):
        pl.loop(0, tiles)(lambda j: mix(s, j))

        @pl.when(s == 0)
        def _():
            run(OPENING[5])
            complete(2)

        @pl.loop(0, 2 * per)
        def _(f):
            slots(s * 2 * per + f, SUMMING)
            share_out(f, mixed, w_out, s, sum_send, sum_recv)

        for i in range(per):
            part_copy(i, s, sum_send, sum_recv).wait_send()
            part_copy(i, s, sum_send, sum_recv).wait_recv()

            @pl.when(s == 0)
            def _():
                toward[i] = summed(i, 0).astype(jnp.bfloat16)
                toward_copy(i).start()

    run(SETTLING[0])
    drain_all((0, 1, 2))
    for i in range(per):
        cols = slice(i * LANES, (i + 1) * LANES)
        toward_copy(i).wait_recv()
        total = summed(i, 1) + inward[i].astype(jnp.float32)
        middle[:, cols] = (x_ref[:, cols].astype(jnp.float32) + total).astype(middle.dtype)
    pair_copy(2, middle, peer.at[0]).start()
    run(SETTLING[1])
    pair_copy(2, middle, peer.at[0]).wait()
    normalize(middle, peer.at[0], ffn_gain, normed.at[0])
    run(SETTLING[2])
    complete(3)
    complete(4)
    units = hidden.shape[1]
    wide = units // LANES

    @pl.loop(0, wide)
    def _(j):
        slots(j, ENDING[:wide])

        @pl.when(j == spans[6][2] // LANES)
        def _():
            complete(6)
            complete(7)
            drain_all((3, 4))

        feed(pl.multiple_of(j * LANES, LANES), LANES)

    for events in ENDING[wide:-1]:
        run(events)
    if units % LANES:
        feed(wide * LANES, units % LANES)
    run(ENDING[-1])

    @pl.loop(0, 2 * depth)
    def _(t):
        for k in range(depth):
            for side, waits in enumerate((landed, landed_across)):
                @pl.when(t == 2 * k + side)
                def _():
                    for p, piece in enumerate(pieces):
                        if piece[0] == 5:
                            waits(p, k)
        s = choose([order[i][0] for i in range(depth)], z)
        for k in range(1, depth):
            s = jnp.where(t // 2 == k, near(k), s)
        f = jnp.where(t % 2 == 0, line(s, y), line(s, 1 - y))
        share_out(f, hidden, w_down, 0, end_send, end_recv)

    for i in range(per):
        cols = slice(i * LANES, (i + 1) * LANES)
        part_copy(i, 0, end_send, end_recv).wait_recv()
        o_ref[:, cols] = (middle[:, cols].astype(jnp.float32) + summed(i, 0)).astype(o_ref.dtype)
    for i in range(per):
        part_copy(i, 0, end_send, end_recv).wait_send()
        toward_copy(i).wait_send()
    drain_all((6, 7, 5))


def fused(depth, stream_in, mix_gain, lin_weight, branch_weight, lin_taps, rate_blocks, admit_blocks, decay_logit,
          mix_out_gain, out_weight, ffn_gain, gate_weight, up_weight, gate_taps, up_taps, down_weight):
    own = stream_in[0]
    length, share = own.shape
    n = LINE * depth
    shards = (lin_weight, branch_weight, out_weight, gate_weight, up_weight, down_weight)
    half = lin_weight.shape[1] // 2
    heights = [half if m == 2 else w.shape[0] for m, w in enumerate(shards)]
    widths = [half if m < 2 else w.shape[1] for m, w in enumerate(shards)]
    spans = blocks(heights, widths)
    pieces = plan(spans)
    bf = jnp.bfloat16
    whole = [
        pltpu.VMEM((n, h, w), bf) if m in (2, 5) else pltpu.VMEM((n * h, w), bf)
        for m, (h, w) in enumerate(zip(heights, widths))
    ]
    units = gate_weight.shape[1]
    width = out_weight.shape[1]
    count = len(pieces)
    dma = pltpu.SemaphoreType.DMA
    scratch = whole + [
        pltpu.VMEM((2, length, share), bf),
        pltpu.VMEM((2, length, 2 * share), bf),
        pltpu.VMEM((length, half), bf),
        pltpu.VMEM((n // 2, length, width), bf),
        pltpu.VMEM((n // 2, length, width), bf),
        pltpu.VMEM((2, n // 2, length, width), bf),
        pltpu.VMEM((length, share), bf),
        pltpu.VMEM((length, units), bf),
        pltpu.VMEM((length, LANES), jnp.float32),
        pltpu.VMEM((length, LANES), jnp.float32),
        pltpu.VMEM((length, share), bf),
        pltpu.VMEM((n // 2, length, width), bf),
        pltpu.VMEM((n // 2, length, width), bf),
        dma((6,)),
        dma((count,)),
        dma((count, depth)),
        dma((count,)),
        dma((count, depth)),
        dma((count,)),
        dma((count, depth)),
        dma((count,)),
        dma((count, depth)),
        dma((3,)),
        dma((3,)),
        dma((2, n // 2)),
        dma((2, n // 2)),
        dma((1, n // 2)),
        dma((1, n // 2)),
        dma,
        dma,
        dma((n // 2,)),
        dma((n // 2,)),
    ]
    near = pl.BlockSpec(memory_space=pltpu.VMEM)
    far = pl.BlockSpec(memory_space=pl.ANY)
    macs = length * share * 2 * (3 * share + 3 * units)
    result = pl.pallas_call(
        functools.partial(layer_body, depth, spans, pieces),
        in_specs=[near, near, far, far, near, near, near, near, near, far, near, far, far, near, near, far],
        out_specs=near,
        out_shape=pltpu.VMEM((length, share), bf),
        scratch_shapes=scratch,
        compiler_params=pltpu.CompilerParams(collective_id=0, has_side_effects=True, vmem_limit_bytes=60000000),
        cost_estimate=pl.CostEstimate(flops=2 * macs, bytes_accessed=2 * macs // length, transcendentals=0),
        name="layer",
    )(own, mix_gain.reshape(1, -1), lin_weight, branch_weight, lin_taps, rate_blocks, admit_blocks, decay_logit.reshape(1, -1),
      mix_out_gain.reshape(1, -1), out_weight, ffn_gain.reshape(1, -1), gate_weight, up_weight, gate_taps,
      up_taps, down_weight)
    return result[None]


def gathered(tps, stream_in, mix_gain, lin_weight, branch_weight, lin_taps, rate_blocks, admit_blocks,
             decay_logit, mix_out_gain, out_weight, ffn_gain, gate_weight, up_weight, gate_taps, up_taps, down_weight):
    own = stream_in[0]
    length, share = own.shape

    def normed_rows(mine, gain):
        pair = lax.all_gather(mine, "tp", axis=0).astype(jnp.float32)
        mean_sq = jnp.sum(pair * pair, axis=(0, 2), keepdims=True) / (tps * share)
        y = (pair * lax.rsqrt(mean_sq + EPS) * gain.reshape(tps, 1, share)).astype(jnp.bfloat16)
        return y.transpose(1, 0, 2).reshape(length, tps * share)

    def product(left, right):
        return jnp.dot(left, right, preferred_element_type=jnp.float32).astype(jnp.bfloat16)

    def scatter(left, right):
        stack = product(left, right).reshape(length, tps, share).transpose(1, 0, 2)
        if tps == 2:
            tp = lax.axis_index("tp")
            mine = lax.dynamic_index_in_dim(stack, tp, 0, keepdims=False)
            other = lax.dynamic_index_in_dim(stack, 1 - tp, 0, keepdims=False)
            other = lax.ppermute(other, "tp", [(0, 1), (1, 0)])
            return mine.astype(jnp.float32) + other.astype(jnp.float32)
        return lax.psum_scatter(stack, "tp", scatter_dimension=0, tiled=False).astype(jnp.float32)

    def gather(w, axis=0):
        return lax.all_gather(w, "fs", axis=axis, tiled=True)

    normed = normed_rows(own, mix_gain)
    linear = product(normed, gather(lin_weight))
    branch = product(normed, gather(branch_weight))
    slope = (-GATE_SCALE * jax.nn.softplus(-decay_logit)).reshape(1, -1)
    mixed = mixer(linear, branch, lin_taps, rate_blocks, admit_blocks, slope, mix_out_gain.reshape(1, -1))
    middle = (own.astype(jnp.float32) + scatter(mixed, gather(out_weight, 1))).astype(jnp.bfloat16)
    normed2 = normed_rows(middle, ffn_gain)
    gate_pre = product(normed2, gather(gate_weight))
    up_pre = product(normed2, gather(up_weight))
    hidden = ffn_gate(gate_pre, up_pre, gate_taps, up_taps)
    result = (middle.astype(jnp.float32) + scatter(hidden, gather(down_weight, 1))).astype(jnp.bfloat16)
    return result[None]


def solution(mesh):
    placed = (
        P(("rep", "fs"), None, "tp"),
        P(),
        P("fs", "tp"),
        P("fs", "tp"),
        P(None, "tp"),
        P("tp", None, None),
        P("tp", None, None),
        P("tp"),
        P("tp"),
        P("tp", "fs"),
        P(),
        P("fs", "tp"),
        P("fs", "tp"),
        P(None, "tp"),
        P(None, "tp"),
        P("tp", "fs"),
    )
    reps, n, tps = mesh.shape["rep"], mesh.shape["fs"], mesh.shape["tp"]
    if reps == 2 and tps == 2 and n == 8:
        body = functools.partial(fused, n // LINE)
    else:
        body = functools.partial(gathered, tps)
    return jax.shard_map(
        body, mesh=mesh, in_specs=placed, out_specs=P(("rep", "fs"), None, "tp"), check_vma=False
    )
```

```python
import functools

import jax
import jax.numpy as jnp
from jax import lax
from jax.experimental import pallas as pl
from jax.experimental.pallas import tpu as pltpu
from jax.sharding import PartitionSpec as P

EPS = 1e-06
GATE_SCALE = 8.0
MESH = pl.DeviceIdType.MESH
LANES = 256
LINE = 2


def shift_rows(x, d, fill):
    rows = lax.broadcasted_iota(jnp.int32, x.shape, 0)
    return jnp.where(rows < d, fill, pltpu.roll(x, d, 0))


def mixer_body(lin_ref, br_ref, taps_ref, rate_ref, admit_ref, slope_ref, gain_ref, o_ref, a_ref, b_ref):
    length, width = lin_ref.shape
    hd = rate_ref.shape[1]
    linear = lin_ref[...].astype(jnp.float32)
    kernel_len = taps_ref.shape[0]
    filtered = linear * taps_ref[kernel_len - 1 : kernel_len]
    for d in range(1, kernel_len):
        filtered = filtered + shift_rows(linear, d, 0.0) * taps_ref[kernel_len - 1 - d : kernel_len - d]
    narrow = filtered.astype(jnp.bfloat16)
    for j in range(width // hd):
        cols = slice(j * hd, (j + 1) * hd)
        piece = narrow[:, cols]
        rate = jax.nn.sigmoid(jnp.dot(piece, rate_ref[j], preferred_element_type=jnp.float32))
        admit = jax.nn.sigmoid(jnp.dot(piece, admit_ref[j], preferred_element_type=jnp.float32))
        log_decay = rate * slope_ref[:, cols]
        u = 2.0 * log_decay
        decay = jnp.exp(log_decay)
        poly = 1.0 + u * (1.0 / 7.0)
        for c in (6.0, 5.0, 4.0, 3.0, 2.0):
            poly = 1.0 + u * (1.0 / c) * poly
        loss = jnp.where(u > -0.35, -u * poly, 1.0 - decay * decay)
        a = decay
        b = jnp.sqrt(loss) * admit * filtered[:, cols]
        sub = lax.broadcasted_iota(jnp.int32, a.shape, 0) % 8
        for d in (1, 2, 4):
            keep = sub >= d
            pa = jnp.where(keep, pltpu.roll(a, d, 0), 1.0)
            pb = jnp.where(keep, pltpu.roll(b, d, 0), 0.0)
            b = a * pb + b
            a = a * pa
        a_ref[:, cols] = a
        b_ref[:, cols] = b

    def advance(t, carry):
        rows = pl.ds(pl.multiple_of(t * 8, 8), 8)
        s = a_ref[rows, :] * carry + b_ref[rows, :]
        b_ref[rows, :] = s
        return s[7:8, :]

    lax.fori_loop(0, length // 8, advance, jnp.zeros((1, width), jnp.float32), unroll=8)
    for j in range(width // hd):
        cols = slice(j * hd, (j + 1) * hd)
        gated = b_ref[:, cols] * jax.nn.gelu(br_ref[:, cols].astype(jnp.float32))
        scale = lax.rsqrt(jnp.mean(gated * gated, axis=-1, keepdims=True) + EPS)
        o_ref[:, cols] = (gated * scale * gain_ref[:, cols]).astype(o_ref.dtype)


def mixer(linear, branch, taps, rate_blocks, admit_blocks, slope, gain):
    length, channels = linear.shape
    hd = rate_blocks.shape[1]
    per = 2 if rate_blocks.shape[0] % 2 == 0 else 1
    width = per * hd
    wide = pl.BlockSpec((length, width), lambda i: (0, i))
    row = pl.BlockSpec((1, width), lambda i: (0, i))
    blk = pl.BlockSpec((per, hd, hd), lambda i: (i, 0, 0))
    return pl.pallas_call(
        mixer_body,
        grid=(channels // width,),
        in_specs=[wide, wide, pl.BlockSpec((taps.shape[0], width), lambda i: (0, i)), blk, blk, row, row],
        out_specs=wide,
        out_shape=jax.ShapeDtypeStruct((length, channels), jnp.bfloat16),
        scratch_shapes=[pltpu.VMEM((length, width), jnp.float32), pltpu.VMEM((length, width), jnp.float32)],
        cost_estimate=pl.CostEstimate(flops=length * channels * 20000, bytes_accessed=length * channels * 6, transcendentals=0),
        name="mixer",
    )(linear, branch, taps, rate_blocks, admit_blocks, slope, gain)


def ffn_body(g_ref, u_ref, gt_ref, ut_ref, o_ref):
    def conv(ref, taps):
        x = ref[...].astype(jnp.float32)
        n = taps.shape[0]
        y = x * taps[n - 1 : n]
        for d in range(1, n):
            y = y + shift_rows(x, d, 0.0) * taps[n - 1 - d : n - d]
        return y

    o_ref[...] = (jax.nn.silu(conv(g_ref, gt_ref)) * conv(u_ref, ut_ref)).astype(o_ref.dtype)


def ffn_gate(gate_pre, up_pre, gate_taps, up_taps):
    length, units = gate_pre.shape
    width = 128
    wide = pl.BlockSpec((length, width), lambda i: (0, i))
    tap = pl.BlockSpec((gate_taps.shape[0], width), lambda i: (0, i))
    return pl.pallas_call(
        ffn_body,
        grid=(units // width,),
        in_specs=[wide, wide, tap, tap],
        out_specs=wide,
        out_shape=jax.ShapeDtypeStruct((length, units), jnp.bfloat16),
        cost_estimate=pl.CostEstimate(flops=length * units * 8000, bytes_accessed=length * units * 6, transcendentals=0),
        name="ffn_gate",
    )(gate_pre, up_pre, gate_taps, up_taps)


SPLIT = (
    ((8, 8,), (8, 8,),),
    ((8, 8,), (8, 8,),),
    ((8, 8,),),
    ((4, 4,),),
    ((4, 4,),),
    ((8, 5,), (8, 4,), (8, 4,), (8, 4,),),
    ((8, 4,),),
    ((8, 8,),),
)
OPENING = (
    ((0, 1, 0,),),
    ((0, 5, 0,), (0, 6, 0,), (0, 0, 0,),),
    ((1, 6, 1,), (0, 2, 0,), (1, 1, 1,), (0, 3, 0,), (0, 12, 0,), (1, 2, 1,), (1, 1, 2,), (1, 6, 2,), (1, 0, 1,), (1, 2, 2,), (1, 6, 3,), (1, 1, 3,), (0, 11, 0,), (1, 0, 2,), (1, 3, 1,), (1, 5, 2,), (1, 3, 2,),),
    ((2, 0, 0,), (1, 5, 1,), (2, 12, 0,), (1, 5, 3,), (2, 5, 0,), (2, 1, 3,), (0, 4, 0,), (2, 6, 2,), (2, 0, 2,), (2, 2, 1,), (2, 6, 0,), (1, 3, 3,), (2, 6, 3,), (2, 0, 1,), (2, 1, 2,), (2, 1, 1,),),
    ((2, 3, 0,), (1, 2, 3,), (1, 0, 3,), (1, 4, 1,), (1, 4, 2,), (2, 3, 2,), (1, 4, 3,), (1, 12, 1,), (1, 11, 1,), (2, 1, 0,), (2, 4, 0,), (2, 2, 0,), (2, 11, 0,), (2, 5, 1,), (2, 2, 2,), (1, 11, 2,), (2, 2, 3,), (2, 3, 3,), (1, 12, 2,), (2, 5, 2,), (2, 3, 1,), (2, 0, 3,), (0, 10, 0,),),
    ((2, 4, 3,),),
)
MIXING = (
    ((), ((2, 5, 3,), (2, 6, 1,),), ((1, 7, 2,),), ((1, 8, 1,), (1, 7, 3,), (2, 10, 0,), (2, 12, 2,),),),
    (((0, 7, 0,), (0, 9, 0,),), ((2, 4, 2,),), ((1, 8, 2,),), (),),
    ((), ((2, 4, 1,), (0, 8, 0,),), (), (),),
)
SUMMING = (
    (),
    (),
    ((2, 12, 1,), (1, 10, 1,),),
    (),
    (),
    ((2, 11, 1,),),
    (),
    ((1, 7, 1,), (2, 11, 2,),),
    (),
    (),
    (),
    (),
    (),
    (),
    (),
    ((1, 12, 3,), (2, 7, 1,), (1, 10, 2,),),
)
SETTLING = (
    ((1, 9, 1,), (2, 7, 0,), (2, 9, 0,), (2, 8, 0,), (2, 7, 2,), (1, 8, 3,),),
    ((2, 8, 2,), (2, 10, 1,), (1, 11, 3,),),
    ((1, 9, 2,),),
)
ENDING = (
    ((2, 7, 3,),),
    (),
    ((1, 10, 3,), (2, 9, 1,), (2, 12, 3,), (2, 8, 1,),),
    ((1, 9, 3,), (2, 8, 3,), (2, 11, 3,), (2, 10, 2,),),
    ((2, 9, 2,),),
    ((2, 10, 3,),),
    ((2, 9, 3,),),
)


def blocks(heights, widths):
    units = widths[3]
    left = -(-units // (2 * LANES)) * LANES
    span = [(m, heights[m], 0, widths[m]) for m in range(6)]
    span[3:5] = [(m, heights[m], 0, left) for m in (3, 4)]
    return span + [(m, heights[m], left, units - left) for m in (3, 4)]


def plan(spans):
    cuts = []
    for b, (_, rows, _, _) in enumerate(spans):
        parts = len(SPLIT[b])
        step = -(-rows // (128 * parts)) * 128
        cuts.append([(b, at, min(step, rows - at)) + SPLIT[b][i] for i, at in enumerate(range(0, rows, step))])
    pieces = []
    for group in ((0, 1), (2,), (3, 4), (6, 7), (5,)):
        for i in range(max(len(cuts[b]) for b in group)):
            pieces += [cuts[b][i] for b in group if i < len(cuts[b])]
    return pieces


def nearest(depth):
    return [sorted(range(depth), key=lambda s: (abs(s - z), -s)) for z in range(depth)]


def choose(values, at):
    out = jnp.int32(values[0])
    for i, v in enumerate(values[1:], 1):
        out = jnp.where(at == i, jnp.int32(v), out)
    return out


def layer_body(depth, spans, pieces, x_hbm, mix_gain, lin_hbm, br_hbm, taps_ref, rate_ref, admit_ref, logit_ref,
               mix_out_gain, out_hbm, ffn_gain, gate_hbm, up_hbm, gtap_ref, utap_ref, down_hbm, o_ref,
               w_lin, w_br, w_out, w_gate, w_up, w_down, peer, normed, mixed, kept, sent, got, middle, hidden,
               a_ref, b_ref, visit, toward, inward, x_ref, local_sem, z_send, z_recv, y_send, y_recv, p_send, p_recv, q_send, q_recv,
               pair_send, pair_recv, sum_send, sum_recv, end_send, end_recv, visit_send, visit_recv, part_send, part_recv):
    x = lax.axis_index("rep")
    f_own = lax.axis_index("fs")
    tp = lax.axis_index("tp")
    z, y = f_own // LINE, f_own % LINE
    length, share = x_ref.shape
    order = nearest(depth)
    hbm = (lin_hbm, br_hbm, out_hbm, gate_hbm, up_hbm, down_hbm)
    full = (w_lin, w_br, w_out, w_gate, w_up, w_down)
    flat = tuple(len(w.shape) == 2 for w in full)
    height = tuple(w.shape[0] // (LINE * depth) if flat[m] else w.shape[1] for m, w in enumerate(full))
    half = w_lin.shape[1]

    def line(s, row):
        return s * LINE + row

    def near(k):
        return choose([order[i][k] for i in range(depth)], z)

    def view(p, f, start, size):
        b, row0 = pieces[p][:2]
        m, _, col, width = spans[b]
        start = pl.multiple_of(row0 + start, 16)
        if flat[m]:
            return full[m].at[pl.ds(pl.multiple_of(f * height[m] + start, 16), size), pl.ds(col, width)]
        return full[m].at[f, pl.ds(start, size), :]

    def parts(p):
        q, (u, v) = pieces[p][2] // 8, pieces[p][3:]
        return {
            "z": ((8 - u) * q * x, u * q),
            "y": ((8 - v) * q * x, v * q),
            "p_out": (u * q * x, (8 - u) * q),
            "p_in": (u * q * (1 - x), (8 - u) * q),
            "q_out": (v * q * x, (8 - v) * q),
            "q_in": (v * q * (1 - x), (8 - v) * q),
        }

    def spare(p, side):
        return pieces[p][3 + side] < 8

    def push(p, f, part, send, recv, device):
        ref = view(p, f, *parts(p)[part])
        return pltpu.make_async_remote_copy(
            src_ref=ref, dst_ref=ref, send_sem=send, recv_sem=recv, device_id=device, device_id_type=MESH
        )

    def own_copy(m):
        src = hbm[m]
        if m < 2:
            src = src.at[:, pl.ds(pl.multiple_of(x * half, LANES), half)]
        if m == 2:
            src = src.at[pl.ds(pl.multiple_of(x * half, LANES), half), :]
        dst = full[m].at[pl.ds(pl.multiple_of(f_own * height[m], 16), height[m]), :] if flat[m] else full[m].at[f_own]
        return pltpu.make_async_copy(src, dst, local_sem.at[m])

    def own(p):
        @pl.when(z < depth - 1)
        def _():
            push(p, f_own, "z", z_send.at[p], z_recv.at[p, z], {"fs": line(z + 1, y)}).start()

        @pl.when(z > 0)
        def _():
            push(p, f_own, "z", z_send.at[p], z_recv.at[p, z], {"fs": line(z - 1, y)}).start()

        push(p, f_own, "y", y_send.at[p], y_recv.at[p, z], {"fs": line(z, 1 - y)}).start()

    def along(p, k):
        s = near(k)
        f = line(s, y)
        push(p, f, "z", z_send.at[p], z_recv.at[p, s], {"fs": f_own}).wait_recv()
        onward = jnp.where(s < z, z + 1, z - 1)

        @pl.when(jnp.logical_and(onward >= 0, onward < depth))
        def _():
            push(p, f, "z", z_send.at[p], z_recv.at[p, s], {"fs": line(onward, y)}).start()

        push(p, f, "y", y_send.at[p], y_recv.at[p, s], {"fs": line(z, 1 - y)}).start()
        if spare(p, 0):
            push(p, f, "p_out", p_send.at[p], p_recv.at[p, s], {"rep": 1 - x}).start()

    def over(p, k):
        s = near(k)
        f = line(s, 1 - y)
        push(p, f, "y", y_send.at[p], y_recv.at[p, s], {"fs": f_own}).wait_recv()
        if spare(p, 1):
            push(p, f, "q_out", q_send.at[p], q_recv.at[p, s], {"rep": 1 - x}).start()

    def landed(p, k):
        s = near(k)
        if k and spare(p, 0):
            push(p, line(s, y), "p_in", p_send.at[p], p_recv.at[p, s], {"rep": 1 - x}).wait_recv()

    def landed_across(p, k):
        s = near(k)
        if spare(p, 1):
            push(p, line(s, 1 - y), "q_in", q_send.at[p], q_recv.at[p, s], {"rep": 1 - x}).wait_recv()

    def complete(m):
        for p, piece in enumerate(pieces):
            if piece[0] == m:
                for k in range(depth):
                    landed(p, k)
                    landed_across(p, k)

    def all_sent(p, part, copies, sem):
        b = pieces[p][0]
        m, _, _, width = spans[b]
        rows = parts(p)[part][1]
        if flat[m]:
            ref = full[m].at[pl.ds(0, copies * rows), pl.ds(0, width)]
        else:
            ref = full[m].at[pl.ds(0, copies), pl.ds(0, rows), :]
        pltpu.make_async_remote_copy(
            src_ref=ref, dst_ref=ref, send_sem=sem, recv_sem=sem, device_id={"rep": 1 - x}, device_id_type=MESH
        ).wait_send()

    def drain(p):
        inner = jnp.logical_and(z > 0, z < depth - 1)
        pl.when(inner)(lambda: all_sent(p, "z", depth + 1, z_send.at[p]))
        pl.when(jnp.logical_not(inner))(lambda: all_sent(p, "z", 1, z_send.at[p]))
        all_sent(p, "y", depth, y_send.at[p])
        if spare(p, 0):
            all_sent(p, "p_out", depth - 1, p_send.at[p])
        if spare(p, 1):
            all_sent(p, "q_out", depth, q_send.at[p])

    def drain_all(blocks_done):
        for p, piece in enumerate(pieces):
            if piece[0] in blocks_done:
                drain(p)

    def run(events):
        for kind, p, k in events:
            if kind == 0:
                own(p)
            elif kind == 1:
                along(p, k)
            else:
                over(p, k)

    def slots(step, groups):
        for i, events in enumerate(groups):
            if events:
                pl.when(step == i)(functools.partial(run, events))

    def pair_copy(i, src, dst):
        return pltpu.make_async_remote_copy(
            src_ref=src, dst_ref=dst, send_sem=pair_send.at[i], recv_sem=pair_recv.at[i],
            device_id={"tp": 1 - tp}, device_id_type=MESH,
        )

    def normalize(mine, theirs, gain, target):
        def chunk(i, carry):
            rows = pl.ds(pl.multiple_of(i * 128, 128), 128)
            a = mine[rows, :].astype(jnp.float32)
            b = theirs[rows, :].astype(jnp.float32)
            total = jnp.sum(a * a, axis=-1, keepdims=True) + jnp.sum(b * b, axis=-1, keepdims=True)
            scale = lax.rsqrt(total / (2 * share) + EPS)
            here = pl.ds(pl.multiple_of(tp * share, LANES), share)
            there = pl.ds(pl.multiple_of((1 - tp) * share, LANES), share)
            target[rows, here] = (a * scale * gain[:, here]).astype(jnp.bfloat16)
            target[rows, there] = (b * scale * gain[:, there]).astype(jnp.bfloat16)
            return carry

        lax.fori_loop(0, length // 128, chunk, 0)

    def project(left, right):
        return jnp.dot(left, right, preferred_element_type=jnp.float32).astype(jnp.bfloat16)

    tiles = half // LANES

    def mix(s, j):
        cols = pl.ds(pl.multiple_of(j * LANES, LANES), LANES)
        wide = pl.ds(pl.multiple_of(x * half + j * LANES, LANES), LANES)
        hd = rate_ref.shape[1]
        step = s * tiles + j
        slots(step, MIXING[0])
        linear = project(normed[s], w_lin[:, cols]).astype(jnp.float32)
        kernel_len = taps_ref.shape[0]
        filtered = linear * taps_ref[kernel_len - 1 : kernel_len, wide]
        for d in range(1, kernel_len):
            filtered = filtered + shift_rows(linear, d, 0.0) * taps_ref[kernel_len - 1 - d : kernel_len - d, wide]
        narrow = filtered.astype(jnp.bfloat16)
        for i in range(LANES // hd):
            part = slice(i * hd, (i + 1) * hd)
            lanes = pl.ds(pl.multiple_of(x * half + j * LANES + i * hd, hd), hd)
            block = x * (half // hd) + j * (LANES // hd) + i
            piece = narrow[:, part]
            rate = jax.nn.sigmoid(jnp.dot(piece, rate_ref[block], preferred_element_type=jnp.float32))
            admit = jax.nn.sigmoid(jnp.dot(piece, admit_ref[block], preferred_element_type=jnp.float32))
            logit = logit_ref[:, lanes]
            slope = -GATE_SCALE * (jnp.maximum(-logit, 0.0) + jnp.log1p(jnp.exp(-jnp.abs(logit))))
            log_decay = rate * slope
            u = 2.0 * log_decay
            a = jnp.exp(log_decay)
            poly = 1.0 + u * (1.0 / 7.0)
            for c in (6.0, 5.0, 4.0, 3.0, 2.0):
                poly = 1.0 + u * (1.0 / c) * poly
            loss = jnp.where(u > -0.35, -u * poly, 1.0 - a * a)
            b = jnp.sqrt(loss) * admit * filtered[:, part]
            sub = lax.broadcasted_iota(jnp.int32, a.shape, 0) % 8
            for d in (1, 2, 4):
                keep = sub >= d
                pa = jnp.where(keep, pltpu.roll(a, d, 0), 1.0)
                pb = jnp.where(keep, pltpu.roll(b, d, 0), 0.0)
                b = a * pb + b
                a = a * pa
            a_ref[:, part] = a
            b_ref[:, part] = b
        slots(step, MIXING[1])

        def advance(t, carry):
            rows = pl.ds(pl.multiple_of(t * 8, 8), 8)
            s = a_ref[rows, :] * carry + b_ref[rows, :]
            b_ref[rows, :] = s
            return s[7:8, :]

        lax.fori_loop(0, length // 8, advance, jnp.zeros((1, LANES), jnp.float32), unroll=8)
        slots(step, MIXING[2])
        branch = project(normed[s], w_br[:, cols])
        for i in range(LANES // hd):
            part = slice(i * hd, (i + 1) * hd)
            lanes = pl.ds(pl.multiple_of(x * half + j * LANES + i * hd, hd), hd)
            local = pl.ds(pl.multiple_of(j * LANES + i * hd, hd), hd)
            gated = b_ref[:, part] * jax.nn.gelu(branch[:, part].astype(jnp.float32))
            scale = lax.rsqrt(jnp.mean(gated * gated, axis=-1, keepdims=True) + EPS)
            mixed[:, local] = (gated * scale * mix_out_gain[:, lanes]).astype(mixed.dtype)

    def feed(col, width):
        cols = pl.ds(col, width)

        def conv(weight, taps):
            v = project(normed[0], weight[:, cols]).astype(jnp.float32)
            n = taps.shape[0]
            out = v * taps[n - 1 : n, cols]
            for d in range(1, n):
                out = out + shift_rows(v, d, 0.0) * taps[n - 1 - d : n - d, cols]
            return out

        hidden[:, cols] = (jax.nn.silu(conv(w_gate, gtap_ref)) * conv(w_up, utap_ref)).astype(hidden.dtype)

    per = kept.shape[0]

    def share_out(f, left, weight, s, send, recv):
        result = project(left[...], weight[f])
        slot = f % per

        @pl.when(f // per == tp)
        def _():
            kept[slot] = result

        @pl.when(f // per != tp)
        def _():
            sent[slot] = result
            part_copy(slot, s, send, recv).start()

    def part_copy(slot, s, send, recv):
        return pltpu.make_async_remote_copy(
            src_ref=sent.at[slot], dst_ref=got.at[s, slot], send_sem=send.at[s, slot], recv_sem=recv.at[s, slot],
            device_id={"tp": 1 - tp}, device_id_type=MESH,
        )

    def swap_copy(src, dst, send, recv):
        return pltpu.make_async_remote_copy(
            src_ref=src, dst_ref=dst, send_sem=send, recv_sem=recv, device_id={"rep": 1 - x}, device_id_type=MESH
        )

    def visit_copy():
        return swap_copy(x_hbm, visit, visit_send, visit_recv)

    def toward_copy(i):
        return swap_copy(toward.at[i], inward.at[i], part_send.at[i], part_recv.at[i])

    def summed(i, s):
        return kept[i].astype(jnp.float32) + got[s, i].astype(jnp.float32)

    for m in range(6):
        own_copy(m).start()
    pltpu.make_async_copy(x_hbm, x_ref, local_sem.at[6]).start()
    barrier = pltpu.get_barrier_semaphore()
    for device in ({"rep": 1 - x}, {"fs": line(z, 1 - y)}, {"tp": 1 - tp}):
        pl.semaphore_signal(barrier, inc=1, device_id=device, device_id_type=MESH)

    @pl.when(z > 0)
    def _():
        pl.semaphore_signal(barrier, inc=1, device_id={"fs": line(z - 1, y)}, device_id_type=MESH)

    @pl.when(z < depth - 1)
    def _():
        pl.semaphore_signal(barrier, inc=1, device_id={"fs": line(z + 1, y)}, device_id_type=MESH)

    pl.semaphore_wait(barrier, 3 + jnp.where(z > 0, 1, 0) + jnp.where(z < depth - 1, 1, 0))

    ready = []

    def prepare(events):
        for event in events:
            m = spans[pieces[event[1]][0]][0]
            if event[0] == 0 and m not in ready:
                own_copy(m).wait()
                ready.append(m)
            run((event,))

    prepare(OPENING[0])
    visit_copy().start()
    pair_copy(0, x_hbm, peer.at[0]).start()
    prepare(OPENING[1])
    pair_copy(0, x_hbm, peer.at[0]).wait()
    pltpu.make_async_copy(x_hbm, x_ref, local_sem.at[6]).wait()
    normalize(x_ref, peer.at[0], mix_gain, normed.at[1])
    prepare(OPENING[2])
    visit_copy().wait()
    pair_copy(1, visit, peer.at[1]).start()
    prepare(OPENING[3])
    pair_copy(1, visit, peer.at[1]).wait()
    normalize(visit, peer.at[1], mix_gain, normed.at[0])
    prepare(OPENING[4])
    for m in range(6):
        if m not in ready:
            own_copy(m).wait()
    complete(0)
    complete(1)

    @pl.loop(0, 2)
    def _(s):
        pl.loop(0, tiles)(lambda j: mix(s, j))

        @pl.when(s == 0)
        def _():
            run(OPENING[5])
            complete(2)

        @pl.loop(0, 2 * per)
        def _(f):
            slots(s * 2 * per + f, SUMMING)
            share_out(f, mixed, w_out, s, sum_send, sum_recv)

        for i in range(per):
            part_copy(i, s, sum_send, sum_recv).wait_send()
            part_copy(i, s, sum_send, sum_recv).wait_recv()

            @pl.when(s == 0)
            def _():
                toward[i] = summed(i, 0).astype(jnp.bfloat16)
                toward_copy(i).start()

    run(SETTLING[0])
    drain_all((0, 1, 2))
    for i in range(per):
        cols = slice(i * LANES, (i + 1) * LANES)
        toward_copy(i).wait_recv()
        total = summed(i, 1) + inward[i].astype(jnp.float32)
        middle[:, cols] = (x_ref[:, cols].astype(jnp.float32) + total).astype(middle.dtype)
    pair_copy(2, middle, peer.at[0]).start()
    run(SETTLING[1])
    pair_copy(2, middle, peer.at[0]).wait()
    normalize(middle, peer.at[0], ffn_gain, normed.at[0])
    run(SETTLING[2])
    complete(3)
    complete(4)
    units = hidden.shape[1]
    wide = units // LANES

    @pl.loop(0, wide)
    def _(j):
        slots(j, ENDING[:wide])

        @pl.when(j == spans[6][2] // LANES)
        def _():
            complete(6)
            complete(7)
            drain_all((3, 4))

        feed(pl.multiple_of(j * LANES, LANES), LANES)

    for events in ENDING[wide:-1]:
        run(events)
    if units % LANES:
        feed(wide * LANES, units % LANES)
    run(ENDING[-1])

    @pl.loop(0, 2 * depth)
    def _(t):
        for k in range(depth):
            for side, waits in enumerate((landed, landed_across)):
                @pl.when(t == 2 * k + side)
                def _():
                    for p, piece in enumerate(pieces):
                        if piece[0] == 5:
                            waits(p, k)
        s = choose([order[i][0] for i in range(depth)], z)
        for k in range(1, depth):
            s = jnp.where(t // 2 == k, near(k), s)
        f = jnp.where(t % 2 == 0, line(s, y), line(s, 1 - y))
        share_out(f, hidden, w_down, 0, end_send, end_recv)

    for i in range(per):
        cols = slice(i * LANES, (i + 1) * LANES)
        part_copy(i, 0, end_send, end_recv).wait_recv()
        o_ref[:, cols] = (middle[:, cols].astype(jnp.float32) + summed(i, 0)).astype(o_ref.dtype)
    for i in range(per):
        part_copy(i, 0, end_send, end_recv).wait_send()
        toward_copy(i).wait_send()
    drain_all((6, 7, 5))


def fused(depth, stream_in, mix_gain, lin_weight, branch_weight, lin_taps, rate_blocks, admit_blocks, decay_logit,
          mix_out_gain, out_weight, ffn_gain, gate_weight, up_weight, gate_taps, up_taps, down_weight):
    own = stream_in[0]
    length, share = own.shape
    n = LINE * depth
    shards = (lin_weight, branch_weight, out_weight, gate_weight, up_weight, down_weight)
    half = lin_weight.shape[1] // 2
    heights = [half if m == 2 else w.shape[0] for m, w in enumerate(shards)]
    widths = [half if m < 2 else w.shape[1] for m, w in enumerate(shards)]
    spans = blocks(heights, widths)
    pieces = plan(spans)
    bf = jnp.bfloat16
    whole = [
        pltpu.VMEM((n, h, w), bf) if m in (2, 5) else pltpu.VMEM((n * h, w), bf)
        for m, (h, w) in enumerate(zip(heights, widths))
    ]
    units = gate_weight.shape[1]
    width = out_weight.shape[1]
    count = len(pieces)
    dma = pltpu.SemaphoreType.DMA
    scratch = whole + [
        pltpu.VMEM((2, length, share), bf),
        pltpu.VMEM((2, length, 2 * share), bf),
        pltpu.VMEM((length, half), bf),
        pltpu.VMEM((n // 2, length, width), bf),
        pltpu.VMEM((n // 2, length, width), bf),
        pltpu.VMEM((2, n // 2, length, width), bf),
        pltpu.VMEM((length, share), bf),
        pltpu.VMEM((length, units), bf),
        pltpu.VMEM((length, LANES), jnp.float32),
        pltpu.VMEM((length, LANES), jnp.float32),
        pltpu.VMEM((length, share), bf),
        pltpu.VMEM((n // 2, length, width), bf),
        pltpu.VMEM((n // 2, length, width), bf),
        pltpu.VMEM((length, share), bf),
        dma((7,)),
        dma((count,)),
        dma((count, depth)),
        dma((count,)),
        dma((count, depth)),
        dma((count,)),
        dma((count, depth)),
        dma((count,)),
        dma((count, depth)),
        dma((3,)),
        dma((3,)),
        dma((2, n // 2)),
        dma((2, n // 2)),
        dma((1, n // 2)),
        dma((1, n // 2)),
        dma,
        dma,
        dma((n // 2,)),
        dma((n // 2,)),
    ]
    near = pl.BlockSpec(memory_space=pltpu.VMEM)
    far = pl.BlockSpec(memory_space=pl.ANY)
    macs = length * share * 2 * (3 * share + 3 * units)
    result = pl.pallas_call(
        functools.partial(layer_body, depth, spans, pieces),
        in_specs=[far, near, far, far, near, near, near, near, near, far, near, far, far, near, near, far],
        out_specs=near,
        out_shape=pltpu.VMEM((length, share), bf),
        scratch_shapes=scratch,
        compiler_params=pltpu.CompilerParams(collective_id=0, has_side_effects=True, vmem_limit_bytes=60000000),
        cost_estimate=pl.CostEstimate(flops=2 * macs, bytes_accessed=2 * macs // length, transcendentals=0),
        name="layer",
    )(own, mix_gain.reshape(1, -1), lin_weight, branch_weight, lin_taps, rate_blocks, admit_blocks, decay_logit.reshape(1, -1),
      mix_out_gain.reshape(1, -1), out_weight, ffn_gain.reshape(1, -1), gate_weight, up_weight, gate_taps,
      up_taps, down_weight)
    return result[None]


def gathered(tps, stream_in, mix_gain, lin_weight, branch_weight, lin_taps, rate_blocks, admit_blocks,
             decay_logit, mix_out_gain, out_weight, ffn_gain, gate_weight, up_weight, gate_taps, up_taps, down_weight):
    own = stream_in[0]
    length, share = own.shape

    def normed_rows(mine, gain):
        pair = lax.all_gather(mine, "tp", axis=0).astype(jnp.float32)
        mean_sq = jnp.sum(pair * pair, axis=(0, 2), keepdims=True) / (tps * share)
        y = (pair * lax.rsqrt(mean_sq + EPS) * gain.reshape(tps, 1, share)).astype(jnp.bfloat16)
        return y.transpose(1, 0, 2).reshape(length, tps * share)

    def product(left, right):
        return jnp.dot(left, right, preferred_element_type=jnp.float32).astype(jnp.bfloat16)

    def scatter(left, right):
        stack = product(left, right).reshape(length, tps, share).transpose(1, 0, 2)
        if tps == 2:
            tp = lax.axis_index("tp")
            mine = lax.dynamic_index_in_dim(stack, tp, 0, keepdims=False)
            other = lax.dynamic_index_in_dim(stack, 1 - tp, 0, keepdims=False)
            other = lax.ppermute(other, "tp", [(0, 1), (1, 0)])
            return mine.astype(jnp.float32) + other.astype(jnp.float32)
        return lax.psum_scatter(stack, "tp", scatter_dimension=0, tiled=False).astype(jnp.float32)

    def gather(w, axis=0):
        return lax.all_gather(w, "fs", axis=axis, tiled=True)

    normed = normed_rows(own, mix_gain)
    linear = product(normed, gather(lin_weight))
    branch = product(normed, gather(branch_weight))
    slope = (-GATE_SCALE * jax.nn.softplus(-decay_logit)).reshape(1, -1)
    mixed = mixer(linear, branch, lin_taps, rate_blocks, admit_blocks, slope, mix_out_gain.reshape(1, -1))
    middle = (own.astype(jnp.float32) + scatter(mixed, gather(out_weight, 1))).astype(jnp.bfloat16)
    normed2 = normed_rows(middle, ffn_gain)
    gate_pre = product(normed2, gather(gate_weight))
    up_pre = product(normed2, gather(up_weight))
    hidden = ffn_gate(gate_pre, up_pre, gate_taps, up_taps)
    result = (middle.astype(jnp.float32) + scatter(hidden, gather(down_weight, 1))).astype(jnp.bfloat16)
    return result[None]


def solution(mesh):
    placed = (
        P(("rep", "fs"), None, "tp"),
        P(),
        P("fs", "tp"),
        P("fs", "tp"),
        P(None, "tp"),
        P("tp", None, None),
        P("tp", None, None),
        P("tp"),
        P("tp"),
        P("tp", "fs"),
        P(),
        P("fs", "tp"),
        P("fs", "tp"),
        P(None, "tp"),
        P(None, "tp"),
        P("tp", "fs"),
    )
    reps, n, tps = mesh.shape["rep"], mesh.shape["fs"], mesh.shape["tp"]
    if reps == 2 and tps == 2 and n == 8:
        body = functools.partial(fused, n // LINE)
    else:
        body = functools.partial(gathered, tps)
    return jax.shard_map(
        body, mesh=mesh, in_specs=placed, out_specs=P(("rep", "fs"), None, "tp"), check_vma=False
    )
```
